32 devices in a mesh: rep: 2 (over x), fs: 8 (over z, y), tp: 2 (over core).
Axes of the slice: x: 2, y: 2, z: 4, core: 2. Of those that a mesh axis runs over, the one named last changes fastest.
Arguments:
- tokens: bfloat16 [8192, 2048], P(('rep', 'fs')), may hold values from -6 to 6
- mixer_gain: float32 [2048], replicated, may hold values from 0.1 to 1.9
- pool_input: float32 [2048, 1024], P('fs', 'tp'), may hold values from -0.125 to 0.125
- input_scale: float32 [1024], P('tp'), may hold values from 0.5 to 2
- group_mix: float32 [128, 1024], P(None, 'tp'), may hold values from -0.5 to 0.5
- group_scale: float32 [1024], P('tp'), may hold values from 0.5 to 2
- pool_output: float32 [2048, 1024], P('fs', 'tp'), may hold values from -0.1875 to 0.1875
- output_scale: float32 [2048], P('fs'), may hold values from 0.5 to 2
- channel_gain: float32 [2048], replicated, may hold values from 0.1 to 1.9
- gate_weight: float32 [2048, 5632], P('fs', 'tp'), may hold values from -0.125 to 0.125
- gate_scale: float32 [5632], P('tp'), may hold values from 0.5 to 2
- up_weight: float32 [2048, 5632], P('fs', 'tp'), may hold values from -0.125 to 0.125
- up_scale: float32 [5632], P('tp'), may hold values from 0.5 to 2
- down_weight: float32 [2048, 5632], P('fs', 'tp'), may hold values from -0.078125 to 0.078125
- down_scale: float32 [2048], P('fs'), may hold values from 0.5 to 2
Outputs:
- layer_out: bfloat16 [8192, 2048], P(('rep', 'fs'))
The draws below stay inside these ranges and needn't reach their ends.
All inputs are finite; a program needn't handle non-finite values.
Results may differ from the reference program's by a relative error of at most 0.02.
Values may be sent and summed in bfloat16 or wider, within the bound.
A program may use at most 128 MiB of HBM per device.

```python
import math
import jax
import jax.numpy as jnp
from jax import lax

D = 2048
FF = 5632
POOL_GROUP = 256
MAP_WIDTH = 128
POOL_WIDTH = 1024
SEQ = 512
TOKENS = 8192
N_TP = 2


def block_levels(stream_key, shape, cuts, smallest, high):
    gain = 1.0
    for dim, parts in cuts:
        draws = jax.random.uniform(jax.random.fold_in(jax.random.fold_in(stream_key, 6), dim), (parts,), jnp.float32, smallest / len(cuts), high / len(cuts))
        gain = gain * jnp.repeat(jnp.exp(draws), shape[dim] // parts).reshape((-1,) + (1,) * (len(shape) - 1 - dim))
    return gain


def normal_values(stream_key, extent, width, bound, shards=(), kind=jnp.bfloat16):
    entries = width * jax.random.normal(stream_key, extent, jnp.float32)
    if shards:
        entries = entries * block_levels(stream_key, extent, shards, -0.22, 0.18)
    return jnp.clip(entries, -bound, bound).astype(kind)


def setup_inputs(seed: int = 0) -> dict:
    key_list = jax.random.split(jax.random.key(seed), 16)
    return {
        "tokens": normal_values(key_list[0], (TOKENS, D), 1.0, 6.0, ((0, 16),)),
        "mixer_gain": jnp.clip(1.0 + 0.18 * jax.random.normal(key_list[1], (D,), jnp.float32), 0.1, 1.9),
        "pool_input": normal_values(key_list[2], (D, POOL_WIDTH), D ** -0.5, 0.125, ((0, 8), (1, 2)), jnp.float32),
        "input_scale": jnp.clip(jnp.exp(math.log(2.0) - 1.3862944 * jax.random.uniform(key_list[3], (POOL_WIDTH,), jnp.float32) ** block_levels(key_list[3], (POOL_WIDTH,), ((0, 2),), -0.2, 0.2)), 0.5, 2.0),
        "group_mix": normal_values(key_list[4], (MAP_WIDTH, POOL_WIDTH), MAP_WIDTH ** -0.5, 0.5, ((1, 2),), jnp.float32),
        "group_scale": jnp.clip(jnp.exp(math.log(2.0) - 1.3862944 * jax.random.uniform(key_list[5], (POOL_WIDTH,), jnp.float32) ** block_levels(key_list[5], (POOL_WIDTH,), ((0, 2),), -0.2, 0.2)), 0.5, 2.0),
        "pool_output": normal_values(key_list[6], (D, POOL_WIDTH), POOL_WIDTH ** -0.5, 0.1875, ((0, 8), (1, 2)), jnp.float32),
        "output_scale": jnp.clip(jnp.exp(math.log(2.0) - 1.3862944 * jax.random.uniform(key_list[7], (D,), jnp.float32) ** block_levels(key_list[7], (D,), ((0, 8),), -0.2, 0.2)), 0.5, 2.0),
        "channel_gain": jnp.clip(1.0 + 0.18 * jax.random.normal(key_list[8], (D,), jnp.float32), 0.1, 1.9),
        "gate_weight": normal_values(key_list[9], (D, FF), D ** -0.5, 0.125, ((0, 8), (1, 2)), jnp.float32),
        "gate_scale": jnp.clip(jnp.exp(math.log(2.0) - 1.3862944 * jax.random.uniform(key_list[10], (FF,), jnp.float32) ** block_levels(key_list[10], (FF,), ((0, 2),), -0.2, 0.2)), 0.5, 2.0),
        "up_weight": normal_values(key_list[11], (D, FF), D ** -0.5, 0.125, ((0, 8), (1, 2)), jnp.float32),
        "up_scale": jnp.clip(jnp.exp(math.log(2.0) - 1.3862944 * jax.random.uniform(key_list[12], (FF,), jnp.float32) ** block_levels(key_list[12], (FF,), ((0, 2),), -0.2, 0.2)), 0.5, 2.0),
        "down_weight": normal_values(key_list[13], (D, FF), FF ** -0.5, 0.078125, ((0, 8), (1, 2)), jnp.float32),
        "down_scale": jnp.clip(jnp.exp(math.log(2.0) - 1.3862944 * jax.random.uniform(key_list[14], (D,), jnp.float32) ** block_levels(key_list[14], (D,), ((0, 8),), -0.2, 0.2)), 0.5, 2.0),
    }


epsilon = 1e-06

def rms_norm(row_block, gain_row):
    floats = row_block.astype(jnp.float32)
    scaled = floats * lax.rsqrt(lax.optimization_barrier(jnp.mean(floats * floats, axis=-1, keepdims=True)) + epsilon)
    return (scaled * gain_row).astype(jnp.bfloat16)

def block_sum(left_rows, weight_rows, feature_scale, blocks):
    length = left_rows.shape[0]
    block_width = left_rows.shape[1] // blocks
    left_split = left_rows.astype(jnp.float32).reshape(length, blocks, block_width)
    right_split = weight_rows.astype(jnp.bfloat16).astype(jnp.float32).reshape(weight_rows.shape[0], blocks, block_width)
    partials = jnp.einsum('sjc,djc->jsd', left_split, right_split)
    rounded = (partials * feature_scale).astype(jnp.bfloat16)
    rounded = lax.optimization_barrier(rounded)
    return lax.optimization_barrier(jnp.sum(rounded.astype(jnp.float32), axis=0))

def one_layer(row_block, mixer_gain, pool_input, input_scale, group_mix, group_scale, pool_output, output_scale, channel_gain, gate_weight, gate_scale, up_weight, up_scale, down_weight, down_scale):
    length = row_block.shape[0]
    normed = rms_norm(row_block, mixer_gain)
    pool_in = (jnp.dot(normed, pool_input.astype(jnp.bfloat16), preferred_element_type=jnp.float32) * input_scale).astype(jnp.bfloat16)
    grouped_in = pool_in.astype(jnp.float32).reshape(length, 4, POOL_GROUP)
    running = jnp.concatenate([jnp.zeros((1, 4, POOL_GROUP), jnp.float32), jnp.cumsum(grouped_in, axis=0)], axis=0)
    places = jnp.arange(length, dtype=jnp.int32)
    window_means = []
    for group_index in range(4):
        window = 2 ** (group_index + 1)
        first_row = jnp.maximum(places + 1 - window, 0).astype(jnp.int32)
        counts = (places + 1 - first_row).astype(jnp.float32)
        window_sum = running[1:, group_index] - running[first_row, group_index]
        window_means.append(window_sum / counts[:, None] - grouped_in[:, group_index])
    pooled = jnp.stack(window_means, axis=1).astype(jnp.bfloat16).reshape(length, POOL_WIDTH)
    map_blocks = POOL_WIDTH // MAP_WIDTH
    mix_matrix = group_mix.astype(jnp.bfloat16).astype(jnp.float32).reshape(MAP_WIDTH, map_blocks, MAP_WIDTH)
    mixed_raw = jnp.einsum('sgc,cgd->sgd', pooled.astype(jnp.float32).reshape(length, map_blocks, MAP_WIDTH), mix_matrix).reshape(length, POOL_WIDTH)
    grouped = (mixed_raw * group_scale).astype(jnp.bfloat16)
    mixer_out = block_sum(grouped, pool_output, output_scale, N_TP)
    middle = (row_block.astype(jnp.float32) + mixer_out).astype(jnp.bfloat16)
    second = rms_norm(middle, channel_gain)
    gate_sum = jnp.dot(second, gate_weight.astype(jnp.bfloat16), preferred_element_type=jnp.float32) * gate_scale
    up_sum = jnp.dot(second, up_weight.astype(jnp.bfloat16), preferred_element_type=jnp.float32) * up_scale
    hidden = (jax.nn.silu(gate_sum) * up_sum).astype(jnp.bfloat16)
    channel_out = block_sum(hidden, down_weight, down_scale, N_TP)
    return (middle.astype(jnp.float32) + channel_out).astype(jnp.bfloat16)

def reference(tokens, mixer_gain, pool_input, input_scale, group_mix, group_scale, pool_output, output_scale, channel_gain, gate_weight, gate_scale, up_weight, up_scale, down_weight, down_scale):
    sequences = tokens.reshape(TOKENS // SEQ, SEQ, D)

    def each_sequence(row_block):
        return one_layer(row_block, mixer_gain, pool_input, input_scale, group_mix, group_scale, pool_output, output_scale, channel_gain, gate_weight, gate_scale, up_weight, up_scale, down_weight, down_scale)
    results = lax.map(each_sequence, sequences)
    return results.reshape(TOKENS, D)
```

```python
import functools

import jax
import jax.numpy as jnp
from jax import lax
from jax.experimental import pallas as pl
from jax.experimental.pallas import tpu as pltpu
from jax.sharding import PartitionSpec as P

POOL_GROUP = 256

epsilon = 1e-06


def normed_rows(floats, gain_row):
    scaled = floats * lax.rsqrt(jnp.mean(floats * floats, axis=-1, keepdims=True) + epsilon)
    return (scaled * gain_row).astype(jnp.bfloat16)


def product(left_rows, weight):
    return jnp.dot(left_rows, weight, preferred_element_type=jnp.float32)


def transposed_product(left_rows, weight_rows):
    return lax.dot_general(
        left_rows, weight_rows, (((1,), (1,)), ((), ())), preferred_element_type=jnp.float32
    )


def thirds(scale):
    high = lax.reduce_precision(scale, 8, 7)
    rest = scale - high
    middle = lax.reduce_precision(rest, 8, 7)
    return [piece.astype(jnp.bfloat16) for piece in (high, middle, rest - middle)]


def make_body(reps, shards, cores):
    def over_rep(value):
        return lax.ppermute(value, "rep", [(i, (i + 1) % reps) for i in range(reps)])

    def over_pair(value):
        return lax.ppermute(value, "fs", [(i, i ^ 1) for i in range(shards)])

    def over_cores(value):
        return lax.ppermute(value, "tp", [(0, 1), (1, 0)])

    def sum_cores(value):
        if cores == 2:
            core = lax.axis_index("tp")
            rows = value.shape[0] // 2
            other = lax.dynamic_slice_in_dim(value, (1 - core) * rows, rows, 0)
            own = lax.dynamic_slice_in_dim(value, core * rows, rows, 0)
            other = lax.ppermute(other.astype(jnp.bfloat16), "tp", [(0, 1), (1, 0)])
            own = lax.optimization_barrier(own.astype(jnp.bfloat16))
            return own.astype(jnp.float32) + other.astype(jnp.float32)
        total = lax.psum_scatter(
            value.astype(jnp.bfloat16), "tp", scatter_dimension=0, tiled=True
        )
        return total.astype(jnp.float32)

    def gather_cores(value):
        if cores == 2:
            core = lax.axis_index("tp")
            other = lax.ppermute(value, "tp", [(0, 1), (1, 0)])
            first = jnp.where(core == 0, value, other)
            second = jnp.where(core == 0, other, value)
            return jnp.concatenate([first, second], axis=0)
        return lax.all_gather(value, "tp", axis=0, tiled=True)

    lines = [[i for i in range(shards) if i % 2 == side] for side in range(2)]

    def body(
        tokens,
        mixer_gain,
        pool_input,
        input_scale,
        group_mix,
        group_scale,
        pool_output,
        output_scale,
        channel_gain,
        gate_weight,
        gate_scale,
        up_weight,
        up_scale,
        down_weight,
        down_scale,
    ):
        rep = lax.axis_index("rep")
        side = lax.axis_index("fs") % 2
        core = lax.axis_index("tp")
        length = tokens.shape[0]
        block_width = group_mix.shape[0]
        local_width = group_mix.shape[1]

        def arranged(own, peer):
            low = jnp.where(side == 0, own, peer)
            high = jnp.where(side == 0, peer, own)
            return low, high

        def share_of(weight, which):
            share = weight.shape[-1] // (2 * reps)
            return lax.dynamic_slice_in_dim(
                weight, (rep * 2 + which) * share, share, weight.ndim - 1
            )

        def shares(weights, which):
            return [share_of(weight, which).astype(jnp.bfloat16) for weight in weights]

        def along_line(block):
            return lax.all_gather(block, "fs", axis=0, tiled=True, axis_index_groups=lines)

        columns = jnp.stack(thirds(output_scale) + thirds(down_scale), axis=1)
        columns = jnp.pad(columns, ((0, 0), (0, 128 - columns.shape[1])))
        mixer_weights = (pool_input, pool_output)
        keep = jnp.concatenate(shares(mixer_weights, side) + [columns], axis=1)
        send = jnp.concatenate(shares(mixer_weights, 1 - side) + [columns], axis=1)
        mine = along_line(jnp.concatenate(arranged(keep, over_pair(send)), axis=0))

        channel_weights = (gate_weight, up_weight, down_weight)
        keep = jnp.concatenate(shares(channel_weights, side), axis=1)
        send = jnp.concatenate(shares(channel_weights, 1 - side), axis=1)
        low, high = arranged(keep, over_pair(send))
        width = keep.shape[1] // 3
        block = jnp.concatenate([low[:, : 2 * width], high[:, : 2 * width]], axis=0)
        block, low, high, mine = lax.optimization_barrier(
            (block, low[:, 2 * width :], high[:, 2 * width :], mine)
        )
        gate_up = along_line(block)
        down_parts = [along_line(low), along_line(high)]

        quarter = local_width // 4
        feature = mine[:, 2 * quarter : 2 * quarter + 6].astype(jnp.float32).T
        output_feature = feature[0:1] + feature[1:2] + feature[2:3]
        down_feature = feature[3:4] + feature[4:5] + feature[5:6]
        mine = mine[:, : 2 * quarter]
        by_rep = over_rep(mine)
        by_side = over_pair(mine)
        split = mine.shape[0] // 2
        by_both = jnp.concatenate([over_pair(by_rep[:split]), over_rep(by_side[split:])], axis=0)
        own_low, own_high = arranged(mine, by_side)
        peer_low, peer_high = arranged(by_rep, by_both)
        quarters = [
            jnp.where(rep == 0, own_low, peer_low),
            jnp.where(rep == 0, own_high, peer_high),
            jnp.where(rep == 0, peer_low, own_low),
            jnp.where(rep == 0, peer_high, own_high),
        ]
        input_full = jnp.concatenate([piece[:, :quarter] for piece in quarters], axis=1)
        output_full = jnp.concatenate([piece[:, quarter:] for piece in quarters], axis=1)

        normed = normed_rows(tokens.astype(jnp.float32), mixer_gain)
        pool_in = (product(normed, input_full) * input_scale).astype(jnp.bfloat16)
        places = jnp.arange(length, dtype=jnp.int32)
        window_sums = pool_in.astype(jnp.float32)
        channel_group = (
            core * local_width + jnp.arange(local_width, dtype=jnp.int32)
        ) // POOL_GROUP
        pooled_mean = jnp.zeros((length, local_width), jnp.float32)
        for group_index in range(4):
            window = 2 ** (group_index + 1)
            shift = window // 2
            window_sums = window_sums + jnp.pad(window_sums[:-shift], ((shift, 0), (0, 0)))
            counts = jnp.minimum(places + 1, window).astype(jnp.float32)
            pooled_mean = jnp.where(
                channel_group[None, :] == group_index, window_sums / counts[:, None], pooled_mean
            )
        pooled = (pooled_mean - pool_in.astype(jnp.float32)).astype(jnp.bfloat16)
        local_blocks = local_width // block_width
        mixed_raw = jnp.einsum(
            "sgc,cgd->sgd",
            pooled.reshape(length, local_blocks, block_width),
            group_mix.astype(jnp.bfloat16).reshape(block_width, local_blocks, block_width),
            preferred_element_type=jnp.float32,
        ).reshape(length, local_width)
        grouped = (mixed_raw * group_scale).astype(jnp.bfloat16)
        mixer_out = sum_cores(transposed_product(grouped, output_full) * output_feature)

        rows = length // cores
        own_tokens = lax.dynamic_slice_in_dim(tokens, core * rows, rows, 0)
        middle = (own_tokens.astype(jnp.float32) + mixer_out).astype(jnp.bfloat16)
        middle = lax.optimization_barrier(middle)
        second = normed_rows(middle.astype(jnp.float32), channel_gain)

        from_rep = over_rep(second)
        from_side = over_pair(second)
        half_rows = rows // 2
        corner = jnp.concatenate(
            [over_pair(from_rep[:half_rows]), over_rep(from_side[half_rows:])], axis=0
        )
        member_rows = jnp.concatenate([second, from_rep, from_side, corner], axis=0)
        if cores == 2:
            row_sets = [over_cores(member_rows), member_rows]
        else:
            row_sets = [lax.all_gather(member_rows, "tp", axis=0, tiled=True)]

        def activated(row_set):
            both = product(row_set, gate_up)
            gate_sum = both[:, :width] * share_of(gate_scale, side)
            up_sum = both[:, width:] * share_of(up_scale, side)
            return (jax.nn.silu(gate_sum) * up_sum).astype(jnp.bfloat16)

        hidden_sets = lax.optimization_barrier([activated(row_set) for row_set in row_sets])

        def wide(value):
            return value.astype(jnp.float32)

        def scattered(down_part, hidden_sets):
            partials = [
                transposed_product(hidden, down_part).astype(jnp.bfloat16)
                for hidden in hidden_sets
            ]
            if cores == 2:
                summed = wide(over_cores(partials[0])) + wide(partials[1])
            else:
                summed = wide(
                    lax.psum_scatter(partials[0], "tp", scatter_dimension=0, tiled=True)
                )
            partial = summed.astype(jnp.bfloat16).reshape(4, rows, -1)
            half = partial.shape[2] // 2
            left, right = partial[:, :, :half], partial[:, :, half:]
            left_two = wide(left[0::2]) + wide(over_rep(left[1::2]))
            right_two = wide(right[:2]) + wide(over_pair(right[2:]))
            left_last = wide(over_pair(left_two[1].astype(jnp.bfloat16)))
            right_last = wide(over_rep(right_two[1].astype(jnp.bfloat16)))
            total = jnp.concatenate([left_two[0] + left_last, right_two[0] + right_last], axis=1)
            return total.reshape(rows, shards // 2, -1)

        low_total = scattered(down_parts[0], hidden_sets)
        low_total, hidden_sets = lax.optimization_barrier((low_total, hidden_sets))
        high_total = scattered(down_parts[1], hidden_sets)
        total = jnp.stack([low_total, high_total], axis=2)
        total = total.reshape(rows, -1)
        own_out = (middle.astype(jnp.float32) + total * down_feature).astype(jnp.bfloat16)
        return gather_cores(own_out)

    return body


MESH = pl.DeviceIdType.MESH
LANES = 128


def remote(src, dst, send, recv, device):
    return pltpu.make_async_remote_copy(
        src_ref=src,
        dst_ref=dst,
        send_sem=send,
        recv_sem=recv,
        device_id=device,
        device_id_type=MESH,
    )


def lanes_at(start, width):
    return pl.ds(pl.multiple_of(start, LANES), width)


def layer_kernel(
    planes,
    tok_any,
    gain1,
    in_scale,
    group_scale,
    out_scale,
    gain2,
    gate_scale,
    up_scale,
    down_scale,
    group_mix,
    pool_in_any,
    pool_out_any,
    gate_any,
    up_any,
    down_any,
    out_any,
    tok,
    mix,
    scales,
    normed,
    gu,
    dn,
    gu_out,
    dn_out,
    xb,
    acc,
    hid,
    pool,
    grp,
    mix_send,
    mix_recv,
    mid,
    cs_send,
    cs_recv,
    own,
    bx_send,
    bx_recv,
    by_send,
    by_recv,
    cx_send,
    cx_recv,
    cy_send,
    cy_recv,
    keep_l,
    keep_r,
    last_l,
    last_r,
    outv,
    local_sem,
    mix_recv_sem,
    mix_up,
    mix_down,
    mix_x,
    mix_corner,
    mix_y,
    sc_recv_sem,
    sc_up,
    sc_down,
    gu_recv_sem,
    gu_up,
    gu_down,
    dn_recv_sem,
    dn_up,
    dn_down,
    y_sem,
    half_sem,
    tok_recv,
    tok_send,
    cs_sems,
    b_sems,
    c_sems,
    o_sems,
):
    f32, bf16 = jnp.float32, jnp.bfloat16
    x = lax.axis_index("rep")
    f = lax.axis_index("fs")
    c = lax.axis_index("tp")
    y = lax.rem(f, 2)
    z = lax.div(f, 2)
    shards = 2 * planes
    depth = mix.shape[2]
    quarter = mix.shape[3] // 4
    rows = mid.shape[1]
    length = tok.shape[0]
    span = gu.shape[2]
    wide = span // 2 // LANES * LANES
    narrow = span // 2 - wide
    to_x = (1 - x, f, c)
    to_y = (x, 2 * z + 1 - y, c)
    to_up = (x, f + 2, c)
    to_down = (x, f - 2, c)
    to_core = (x, f, 1 - c)
    peer = 2 * z + 1 - y
    own_q = 2 * x + y
    y_q = 2 * x + 1 - y
    x_q = 2 * (1 - x) + y
    far_q = 2 * (1 - x) + 1 - y
    sends = []

    def start(copy, cond=None):
        if cond is None:
            copy.start()
        else:
            pl.when(cond)(copy.start)
        sends.append((copy, cond))

    stage = {}
    for i, ref in enumerate((gate_any, up_any, down_any)):
        stage[i] = acc.at[pl.ds(i * depth, depth), :]
    loads = [
        pltpu.make_async_copy(pool_in_any, pool.at[pl.ds(0, depth), :], local_sem.at[0]),
        pltpu.make_async_copy(pool_out_any, pool.at[pl.ds(depth, depth), :], local_sem.at[1]),
    ]
    for i, ref in enumerate((gate_any, up_any, down_any)):
        loads.append(
            pltpu.make_async_copy(ref.at[:, lanes_at(x * span, span)], stage[i], local_sem.at[2 + i])
        )
    loads.append(pltpu.make_async_copy(tok_any, tok, local_sem.at[5]))
    for load in loads:
        load.start()

    barrier = pltpu.get_barrier_semaphore()
    for device in (to_x, to_y, to_core):
        pl.semaphore_signal(barrier, inc=1, device_id=device, device_id_type=MESH)

    @pl.when(z > 0)
    def _():
        pl.semaphore_signal(barrier, inc=1, device_id=to_down, device_id_type=MESH)

    @pl.when(z < planes - 1)
    def _():
        pl.semaphore_signal(barrier, inc=1, device_id=to_up, device_id_type=MESH)

    loads[0].wait()
    mix[0, f] = pool[0:depth, :].astype(bf16)
    loads[1].wait()
    mix[1, f] = pool[depth : 2 * depth, :].astype(bf16)
    row_of = lax.broadcasted_iota(jnp.int32, (8, depth), 0)
    scales[f] = jnp.where(row_of == 0, out_scale[...], down_scale[...])
    for d in range(shards):
        dn[d, wide + narrow :, :] = jnp.zeros((dn.shape[1] - wide - narrow, dn.shape[2]), bf16)
    pl.semaphore_wait(
        barrier, 3 + jnp.where(z > 0, 1, 0) + jnp.where(z < planes - 1, 1, 0)
    )

    def mix_at(slot, q):
        return mix.at[:, slot, :, lanes_at(q * quarter, quarter)]

    def piece(kind, slot):
        if kind == "mix":
            return mix_at(slot, own_q), mix_recv_sem.at[slot, own_q], mix_up, mix_down
        if kind == "sc":
            return scales.at[slot], sc_recv_sem.at[slot], sc_up, sc_down
        if kind == "gu":
            return gu.at[slot], gu_recv_sem.at[slot], gu_up, gu_down
        part = dn.at[slot, pl.ds(0, wide + narrow), :]
        return part, dn_recv_sem.at[slot], dn_up, dn_down

    def to_z(kind, slot, up=None, down=None):
        ref, recv, up_sems, down_sems = piece(kind, slot)
        if up is not None:
            start(remote(ref, ref, up_sems.at[slot], recv, to_up), up)
        if down is not None:
            start(remote(ref, ref, down_sems.at[slot], recv, to_down), down)

    def wait_piece(kind, slot, cond=None):
        ref, recv, _, _ = piece(kind, slot)
        copy = remote(ref, ref, local_sem.at[6], recv, to_x)
        if cond is None:
            copy.wait_recv()
        else:
            pl.when(cond)(copy.wait_recv)

    def own_to_z(kind, slot):
        to_z(kind, slot, z < planes - 1, z > 0)

    def hop(kind, k, t, absolute=False, then=None):
        side = t if absolute else lax.rem(y + t, 2)
        for origin, has, up, down in (
            (z - k, z >= k, jnp.logical_and(z >= k, z < planes - 1), None),
            (z + k, z + k < planes, None, jnp.logical_and(z + k < planes, z > 0)),
        ):
            slot = jnp.clip(2 * origin + side, 0, shards - 1)
            wait_piece(kind, slot, has)
            if k < planes - 1:
                to_z(kind, slot, up, down)
            if then is not None:
                then(slot, has)

    mine = mix_at(f, y_q)
    start(remote(mine, mine, mix_y.at[f, y_q], mix_recv_sem.at[f, y_q], to_y))
    own_to_z("mix", f)
    start(remote(scales.at[f], scales.at[f], y_sem.at[0], sc_recv_sem.at[f], to_y))
    own_to_z("sc", f)

    lane = lax.broadcasted_iota(jnp.int32, (depth, LANES), 1)

    def join(gate_tile, up_tile, side):
        shape = gate_tile.shape
        low_lane = lax.broadcasted_iota(jnp.int32, shape, 1) < narrow
        low = jnp.where(low_lane, gate_tile, pltpu.roll(up_tile, narrow, axis=1))
        high = jnp.where(low_lane, pltpu.roll(gate_tile, narrow, axis=1), up_tile)
        return jnp.where(side == 0, low, high)

    shift_of = wide + LANES

    def build_gu(side, write):
        write(0, wide, stage[0][:, lanes_at(side * shift_of, wide)].astype(bf16))
        write(wide, wide, stage[1][:, lanes_at(side * shift_of, wide)].astype(bf16))
        tile = join(stage[0][:, wide : wide + LANES], stage[1][:, wide : wide + LANES], side)
        write(2 * wide, LANES, tile.astype(bf16))

    def build_dn(side, write):
        for j in range(wide // LANES):
            tile = stage[2][:, lanes_at(side * shift_of + j * LANES, LANES)]
            write(j * LANES, LANES, tile.T.astype(bf16))
        tile = stage[2][:, wide : wide + LANES].T
        write(wide, narrow, jnp.where(side == 0, tile[:narrow], tile[narrow:]).astype(bf16))

    def write_gu_out(at, size, value):
        gu_out[:, at : at + size] = value

    def write_gu_own(at, size, value):
        gu[f, :, at : at + size] = value

    def write_dn_out(at, size, value):
        dn_out[at : at + size, :] = value

    def write_dn_own(at, size, value):
        dn[f, at : at + size, :] = value

    loads[2].wait()
    loads[3].wait()
    build_gu(1 - y, write_gu_out)
    wait_piece("mix", peer)
    own_to_z("mix", peer)
    start(remote(gu_out, gu.at[f], y_sem.at[1], gu_recv_sem.at[f], to_y))
    wait_piece("sc", peer)
    own_to_z("sc", peer)

    def spread(slot, has):
        ref = mix_at(slot, own_q)
        start(remote(ref, ref, mix_x.at[slot], mix_recv_sem.at[slot, own_q], to_x), has)
        start(remote(ref, ref, mix_y.at[slot, own_q], mix_recv_sem.at[slot, own_q], to_y), has)

    build_gu(y, write_gu_own)
    for t in range(2):
        hop("mix", 1, t, then=spread)
        hop("sc", 1, t)

    loads[5].wait()
    step_rows = 32

    @pl.loop(0, length // step_rows)
    def _(i):
        at = pl.ds(pl.multiple_of(i * step_rows, step_rows), step_rows)
        floats = tok[at, :].astype(f32)
        scaled = floats * lax.rsqrt(jnp.mean(floats * floats, axis=-1, keepdims=True) + epsilon)
        value = (scaled * gain1[...]).astype(bf16)
        for d in range(shards):
            normed[d, at, :] = value[:, d * depth : (d + 1) * depth]

    for k in range(2, planes):
        for t in range(2):
            hop("mix", k, t, then=spread)
            hop("sc", k, t)
        if k == planes - 2:
            own_to_z("gu", f)
    for q in (own_q, x_q, far_q):
        ref = mix_at(f, q)
        start(remote(ref, ref, mix_y.at[f, q], mix_recv_sem.at[f, q], to_y))

    loads[4].wait()
    build_dn(1 - y, write_dn_out)
    build_dn(y, write_dn_own)
    start(remote(dn_out, dn.at[f, pl.ds(0, wide + narrow), :], y_sem.at[2], dn_recv_sem.at[f], to_y))

    def wait_mix(slot, q, cond=None):
        ref = mix_at(slot, q)
        copy = remote(ref, ref, local_sem.at[6], mix_recv_sem.at[slot, q], to_x)
        if cond is None:
            copy.wait_recv()
        else:
            pl.when(cond)(copy.wait_recv)

    def others(k, t, do):
        for origin, has in ((z - k, z >= k), (z + k, z + k < planes)):
            do(jnp.clip(2 * origin + lax.rem(y + t, 2), 0, shards - 1), has)

    def corner(slot, has):
        wait_mix(slot, y_q, has)
        ref = mix_at(slot, y_q)
        start(remote(ref, ref, mix_corner.at[slot], mix_recv_sem.at[slot, y_q], to_x), has)

    def rest(slot, has):
        wait_mix(slot, x_q, has)
        wait_mix(slot, far_q, has)

    wait_piece("gu", peer)
    own_to_z("gu", peer)
    for k in range(1, planes):
        for t in range(2):
            others(k, 1 - t, corner)
    hop("gu", 1, 0)
    for k in range(1, planes):
        for t in range(2):
            others(k, t, rest)
    for q in (y_q, x_q, far_q):
        wait_mix(peer, q)

    pool[...] = jnp.zeros(pool.shape, f32)

    @pl.loop(0, shards)
    def _(d):
        pool[...] += jnp.dot(normed[d], mix[0, d], preferred_element_type=f32)

    local_width = pool.shape[1]
    place = lax.broadcasted_iota(jnp.int32, (length, LANES), 0)
    for q in range(local_width // LANES):
        at = slice(q * LANES, (q + 1) * LANES)
        value = (pool[:, at] * in_scale[:, at]).astype(bf16).astype(f32)
        group = lax.div(c * local_width + q * LANES, POOL_GROUP)
        sums = value
        mean = jnp.zeros_like(value)
        for index in range(4):
            window = 2 ** (index + 1)
            shift = window // 2
            sums = sums + jnp.where(place >= shift, pltpu.roll(sums, shift, axis=0), 0.0)
            counts = jnp.minimum(place + 1, window).astype(f32)
            mean = jnp.where(group == index, sums / counts, mean)
        pooled = (mean - value).astype(bf16)
        mixed = jnp.dot(pooled, group_mix[:, at].astype(bf16), preferred_element_type=f32)
        grp[:, at] = (mixed * group_scale[:, at]).astype(bf16)

    def mixer_rows(d, core):
        left = grp[pl.ds(pl.multiple_of(core * rows, rows), rows), :]
        value = lax.dot_general(
            left, mix[1, d], (((1,), (1,)), ((), ())), preferred_element_type=f32
        )
        return (value * scales[d, 0:1, :]).astype(bf16)

    @pl.loop(0, shards)
    def _(d):
        mix_send[d] = mixer_rows(d, 1 - c)

    start(remote(mix_send, mix_recv, half_sem.at[0], half_sem.at[1], to_core))
    hop("gu", 1, 1)

    @pl.loop(0, shards)
    def _(d):
        mid[d] = mixer_rows(d, c)

    remote(mix_send, mix_recv, half_sem.at[0], half_sem.at[1], to_core).wait_recv()
    my_rows = pl.ds(pl.multiple_of(c * rows, rows), rows)
    block = c * 4 + 2 * x + y
    for part in range(4):
        size = rows // 4
        at = pl.ds(part * size, size)
        tok_at = pl.ds(pl.multiple_of(c * rows + part * size, size), size)
        squares = jnp.zeros((size, depth), f32)
        for d in range(shards):
            value = (
                tok[tok_at, d * depth : (d + 1) * depth].astype(f32)
                + (mid[d, at, :].astype(f32) + mix_recv[d, at, :].astype(f32))
            ).astype(bf16)
            mid[d, at, :] = value
            wide_value = value.astype(f32)
            squares = squares + wide_value * wide_value
        mean = jnp.sum(squares, axis=-1, keepdims=True) / (shards * depth)
        factor = lax.rsqrt(mean + epsilon)
        to_at = pl.ds(pl.multiple_of(block * rows + part * size, size), size)
        for d in range(shards):
            scaled = mid[d, at, :].astype(f32) * factor
            gain = gain2[:, d * depth : (d + 1) * depth]
            xb[d, to_at, :] = (scaled * gain).astype(bf16)

    half = rows // 2

    def rows_of(core, bx, by, h=None):
        first = (core * 4 + 2 * bx + by) * rows
        if h is None:
            return xb.at[:, pl.ds(pl.multiple_of(first, rows), rows), :]
        return xb.at[:, pl.ds(pl.multiple_of(first + h * half, half), half), :]

    def send_rows(ref, i, j, device):
        start(remote(ref, ref, tok_send.at[i], tok_recv.at[j], device))

    def wait_rows(ref, j):
        remote(ref, ref, local_sem.at[6], tok_recv.at[j], to_x).wait_recv()

    for h in range(2):
        send_rows(rows_of(c, x, y, h), h, h, to_x)
        send_rows(rows_of(c, x, y, 1 - h), 2 + h, 2 + 1 - h, to_y)
    send_rows(rows_of(c, x, y), 4, 6, to_core)
    hop("gu", 2, 0)
    wait_rows(rows_of(c, 1 - x, y, 0), 0)
    send_rows(rows_of(c, 1 - x, y, 0), 5, 4, to_y)
    wait_rows(rows_of(c, x, 1 - y, 1), 3)
    send_rows(rows_of(c, x, 1 - y, 1), 6, 5, to_x)
    wait_rows(rows_of(c, 1 - x, y, 1), 1)
    send_rows(rows_of(c, 1 - x, y), 7, 7, to_core)
    wait_rows(rows_of(c, x, 1 - y, 0), 2)
    send_rows(rows_of(c, x, 1 - y), 8, 8, to_core)
    hop("gu", 2, 1)
    wait_piece("dn", peer)
    own_to_z("dn", 2 * z)
    own_to_z("dn", 2 * z + 1)
    wait_rows(rows_of(c, 1 - x, 1 - y, 0), 4)
    wait_rows(rows_of(c, 1 - x, 1 - y, 1), 5)
    send_rows(rows_of(c, 1 - x, 1 - y), 9, 9, to_core)
    for i, (bx, by) in enumerate(((x, y), (1 - x, y), (x, 1 - y), (1 - x, 1 - y))):
        wait_rows(rows_of(1 - c, bx, by), 6 + i)

    orders = []
    for plane in range(planes):
        near = sorted(range(planes), key=lambda p: (abs(p - plane), p))
        orders.append(near)

    def plane_at(j):
        value = jnp.int32(0)
        for plane in range(planes):
            value = jnp.where(z == plane, orders[plane][j], value)
        return value

    all_rows = xb.shape[1]
    tall = 512
    tile = 2 * LANES
    flat = span // tile

    def gate_up(slot, first):
        @pl.loop(0, all_rows // tall)
        def _(r):
            at = pl.ds(pl.multiple_of(r * tall, tall), tall)
            left = xb[slot, at, :]

            @pl.loop(0, flat)
            def _(n):
                cols = lanes_at(n * tile, tile)
                value = jnp.dot(left, gu[slot, :, cols], preferred_element_type=f32)
                acc[at, cols] = value if first else acc[at, cols] + value

            if flat * tile < span:
                cols = slice(flat * tile, span)
                value = jnp.dot(left, gu[slot, :, cols], preferred_element_type=f32)
                acc[at, cols] = value if first else acc[at, cols] + value

    gate_up(f, True)
    gate_up(peer, False)

    @pl.loop(0, 2 * (planes - 2))
    def _(i):
        base = jnp.int32(0)
        for j in range(1, planes - 1):
            base = jnp.where(lax.div(i, 2) == j - 1, plane_at(j), base)
        gate_up(2 * base + lax.rem(i, 2), False)

    for k in range(1, planes - 1):
        for t in range(2):
            hop("dn", k, t, absolute=True)
    for t in range(2):
        hop("gu", planes - 1, t)
        gate_up(2 * plane_at(planes - 1) + lax.rem(y + t, 2), False)

    gate_at = lanes_at(x * span + y * shift_of, wide)
    joint_at = lanes_at(x * span + wide, LANES)
    joint_scale = join(
        jnp.broadcast_to(gate_scale[:, joint_at], (8, LANES)),
        jnp.broadcast_to(up_scale[:, joint_at], (8, LANES)),
        y,
    )[0:1]
    gate_row = gate_scale[:, gate_at]
    up_row = up_scale[:, gate_at]
    act = 64

    @pl.loop(0, all_rows // act)
    def _(r):
        at = pl.ds(pl.multiple_of(r * act, act), act)
        for j in range(wide // LANES):
            cols = slice(j * LANES, (j + 1) * LANES)
            gate = acc[at, cols] * gate_row[:, cols]
            up = acc[at, wide + j * LANES : wide + (j + 1) * LANES] * up_row[:, cols]
            hid[at, cols] = (gate / (1.0 + jnp.exp(-gate)) * up).astype(bf16)
        both = acc[at, 2 * wide :] * joint_scale
        value = both / (1.0 + jnp.exp(-both)) * pltpu.roll(both, narrow, axis=1)
        keep = lax.broadcasted_iota(jnp.int32, (act, LANES), 1) < narrow
        hid[at, wide:] = jnp.where(keep, value, 0.0).astype(bf16)

    core_rows = all_rows // 2
    two = 2 * rows
    low, high = slice(0, LANES), slice(LANES, 2 * LANES)

    def slot_at(i):
        return 2 * plane_at(i // 2) + i % 2

    def cs_copy(i):
        s = i % 2
        return remote(cs_send.at[s], cs_recv.at[i], cs_sems.at[s], cs_sems.at[2 + i], to_core)

    def bx_copy(i):
        s = i % 2
        return remote(bx_send.at[s], bx_recv.at[i], b_sems.at[0, s], b_sems.at[0, 2 + i], to_x)

    def by_copy(i):
        s = i % 2
        return remote(by_send.at[s], by_recv.at[i], b_sems.at[1, s], b_sems.at[1, 2 + i], to_y)

    def cx_copy(i):
        s = i % 2
        return remote(cx_send.at[s], cx_recv.at[i], c_sems.at[0, s], c_sems.at[0, 2 + i], to_x)

    def cy_copy(i):
        s = i % 2
        return remote(cy_send.at[s], cy_recv.at[i], c_sems.at[1, s], c_sems.at[1, 2 + i], to_y)

    def out_at(i, core):
        d = slot_at(i)
        return out_any.at[pl.ds(pl.multiple_of(core * rows, rows), rows), lanes_at(d * depth, depth)]

    def out_local(i):
        return pltpu.make_async_copy(outv.at[i], out_at(i, c), o_sems.at[0, i])

    def out_remote(i):
        return remote(outv.at[i], out_at(i, c), o_sems.at[1, i], o_sems.at[2, i], to_core)

    def first_stage(i):
        slot = slot_at(i)
        s = i % 2
        if i >= 2:
            cs_copy(i - 2).wait_send()
        weight = dn[slot]

        @pl.loop(0, core_rows // tall)
        def _(r):
            at = pl.ds(pl.multiple_of(r * tall, tall), tall)
            there = pl.ds(pl.multiple_of((1 - c) * core_rows + r * tall, tall), tall)
            cs_send[s, at, :] = jnp.dot(hid[there, :], dn[slot], preferred_element_type=f32).astype(bf16)

        cs_copy(i).start()

        @pl.loop(0, core_rows // tall)
        def _(r):
            at = pl.ds(pl.multiple_of(r * tall, tall), tall)
            here = pl.ds(pl.multiple_of(c * core_rows + r * tall, tall), tall)
            own[at, :] = jnp.dot(hid[here, :], dn[slot], preferred_element_type=f32)

    def block_rows(bx, by):
        return pl.ds(pl.multiple_of((2 * bx + by) * rows, rows), rows)

    def second_stage(i):
        s = i % 2
        cs_copy(i).wait_recv()
        if i >= 2:
            bx_copy(i - 2).wait_send()
            by_copy(i - 2).wait_send()
        for b in range(2):
            at = block_rows(1 - x, b)
            value = own[at, low] + cs_recv[i, at, low].astype(f32)
            bx_send[s, b] = value.astype(bf16)
        bx_copy(i).start()
        for b in range(2):
            at = block_rows(b, 1 - y)
            value = own[at, high] + cs_recv[i, at, high].astype(f32)
            by_send[s, b] = value.astype(bf16)
        by_copy(i).start()
        for b in range(2):
            at = block_rows(x, b)
            keep_l[s, b] = own[at, low] + cs_recv[i, at, low].astype(f32)
            at = block_rows(b, y)
            keep_r[s, b] = own[at, high] + cs_recv[i, at, high].astype(f32)

    def third_stage(i):
        s = i % 2
        if i >= 2:
            cx_copy(i - 2).wait_send()
            cy_copy(i - 2).wait_send()
        bx_copy(i).wait_recv()
        cy_send[s] = (keep_l[s, 1 - y] + bx_recv[i, 1 - y].astype(f32)).astype(bf16)
        cy_copy(i).start()
        by_copy(i).wait_recv()
        cx_send[s] = (keep_r[s, 1 - x] + by_recv[i, 1 - x].astype(f32)).astype(bf16)
        cx_copy(i).start()
        last_l[s] = keep_l[s, y] + bx_recv[i, y].astype(f32)
        last_r[s] = keep_r[s, x] + by_recv[i, x].astype(f32)

    def fourth_stage(i):
        s = i % 2
        d = slot_at(i)
        scale = scales[d, 1:2, :]
        cy_copy(i).wait_recv()
        total = last_l[s] + cy_recv[i].astype(f32)
        outv[i, :, low] = (mid[d, :, low].astype(f32) + total * scale[:, low]).astype(bf16)
        cx_copy(i).wait_recv()
        total = last_r[s] + cx_recv[i].astype(f32)
        outv[i, :, high] = (mid[d, :, high].astype(f32) + total * scale[:, high]).astype(bf16)
        out_remote(i).start()
        out_local(i).start()

    for i in range(shards):
        if i == 2 * (planes - 1):
            for t in range(2):
                pass
        if i >= 2 * (planes - 1):
            hop("dn", planes - 1, i % 2, absolute=True)
        first_stage(i)
        if i >= 2:
            fourth_stage(i - 2)
        if i >= 1:
            third_stage(i - 1)
        second_stage(i)
    fourth_stage(shards - 2)
    third_stage(shards - 1)
    fourth_stage(shards - 1)

    for copy, cond in sends:
        if cond is None:
            copy.wait_send()
        else:
            pl.when(cond)(copy.wait_send)
    for i in (shards - 2, shards - 1):
        for make in (cs_copy, bx_copy, by_copy, cx_copy, cy_copy):
            make(i).wait_send()
    for i in range(shards):
        out_local(i).wait()
        out_remote(i).wait_send()
        remote(outv.at[i], out_at(i, 1 - c), o_sems.at[1, i], o_sems.at[2, i], to_core).wait_recv()


def make_fast(shards):
    planes = shards // 2

    def body(
        tokens,
        mixer_gain,
        pool_input,
        input_scale,
        group_mix,
        group_scale,
        pool_output,
        output_scale,
        channel_gain,
        gate_weight,
        gate_scale,
        up_weight,
        up_scale,
        down_weight,
        down_scale,
    ):
        f32, bf16 = jnp.float32, jnp.bfloat16
        length, width = tokens.shape
        depth, local_width = pool_input.shape
        span = gate_weight.shape[1] // 2
        padded = (span // 2 + LANES - 1) // LANES * LANES
        rows = length // 2
        everything = 8 * rows
        vmem = pl.BlockSpec(memory_space=pltpu.VMEM)
        anywhere = pl.BlockSpec(memory_space=pl.ANY)
        dma = pltpu.SemaphoreType.DMA
        scratch = [
            pltpu.VMEM((length, width), bf16),
            pltpu.VMEM((2, shards, depth, local_width), bf16),
            pltpu.VMEM((shards, 8, depth), f32),
            pltpu.VMEM((shards, length, depth), bf16),
            pltpu.VMEM((shards, depth, span), bf16),
            pltpu.VMEM((shards, padded, depth), bf16),
            pltpu.VMEM((depth, span), bf16),
            pltpu.VMEM((span // 2, depth), bf16),
            pltpu.VMEM((shards, everything, depth), bf16),
            pltpu.VMEM((everything, span), f32),
            pltpu.VMEM((everything, padded), bf16),
            pltpu.VMEM((length, local_width), f32),
            pltpu.VMEM((length, local_width), bf16),
            pltpu.VMEM((shards, rows, depth), bf16),
            pltpu.VMEM((shards, rows, depth), bf16),
            pltpu.VMEM((shards, rows, depth), bf16),
            pltpu.VMEM((2, 4 * rows, depth), bf16),
            pltpu.VMEM((shards, 4 * rows, depth), bf16),
            pltpu.VMEM((4 * rows, depth), f32),
            pltpu.VMEM((2, 2, rows, LANES), bf16),
            pltpu.VMEM((shards, 2, rows, LANES), bf16),
            pltpu.VMEM((2, 2, rows, LANES), bf16),
            pltpu.VMEM((shards, 2, rows, LANES), bf16),
            pltpu.VMEM((2, rows, LANES), bf16),
            pltpu.VMEM((shards, rows, LANES), bf16),
            pltpu.VMEM((2, rows, LANES), bf16),
            pltpu.VMEM((shards, rows, LANES), bf16),
            pltpu.VMEM((2, 2, rows, LANES), f32),
            pltpu.VMEM((2, 2, rows, LANES), f32),
            pltpu.VMEM((2, rows, LANES), f32),
            pltpu.VMEM((2, rows, LANES), f32),
            pltpu.VMEM((shards, rows, depth), bf16),
            dma((7,)),
            dma((shards, 4)),
            dma((shards,)),
            dma((shards,)),
            dma((shards,)),
            dma((shards,)),
            dma((shards, 4)),
            dma((shards,)),
            dma((shards,)),
            dma((shards,)),
            dma((shards,)),
            dma((shards,)),
            dma((shards,)),
            dma((shards,)),
            dma((shards,)),
            dma((shards,)),
            dma((3,)),
            dma((2,)),
            dma((10,)),
            dma((10,)),
            dma((2 + shards,)),
            dma((2, 2 + shards)),
            dma((2, 2 + shards)),
            dma((3, shards)),
        ]
        row = lambda value: value.reshape(1, -1)
        return pl.pallas_call(
            functools.partial(layer_kernel, planes),
            name="layer",
            out_shape=jax.ShapeDtypeStruct((length, width), bf16),
            in_specs=[anywhere] + [vmem] * 9 + [anywhere] * 5,
            out_specs=anywhere,
            scratch_shapes=scratch,
            compiler_params=pltpu.CompilerParams(
                collective_id=0, has_side_effects=True, vmem_limit_bytes=67043328
            ),
        )(
            tokens,
            row(mixer_gain),
            row(input_scale),
            row(group_scale),
            row(output_scale),
            row(channel_gain),
            row(gate_scale),
            row(up_scale),
            row(down_scale),
            group_mix,
            pool_input,
            pool_output,
            gate_weight,
            up_weight,
            down_weight,
        )

    return body


def solution(mesh):
    in_specs = (
        P(("rep", "fs"), None),
        P(),
        P("fs", "tp"),
        P("tp"),
        P(None, "tp"),
        P("tp"),
        P("fs", "tp"),
        P("fs"),
        P(),
        P("fs", "tp"),
        P("tp"),
        P("fs", "tp"),
        P("tp"),
        P("fs", "tp"),
        P("fs"),
    )
    out_specs = P(("rep", "fs"), None)
    reps, shards, cores = mesh.shape["rep"], mesh.shape["fs"], mesh.shape["tp"]
    fast = reps == 2 and cores == 2 and shards % 2 == 0
    body = make_fast(shards) if fast else make_body(reps, shards, cores)
    return jax.shard_map(body, mesh=mesh, in_specs=in_specs, out_specs=out_specs, check_vma=False)
```

```python
import functools

import jax
import jax.numpy as jnp
from jax import lax
from jax.experimental import pallas as pl
from jax.experimental.pallas import tpu as pltpu
from jax.sharding import PartitionSpec as P

POOL_GROUP = 256

epsilon = 1e-06


def normed_rows(floats, gain_row):
    scaled = floats * lax.rsqrt(jnp.mean(floats * floats, axis=-1, keepdims=True) + epsilon)
    return (scaled * gain_row).astype(jnp.bfloat16)


def product(left_rows, weight):
    return jnp.dot(left_rows, weight, preferred_element_type=jnp.float32)


def transposed_product(left_rows, weight_rows):
    return lax.dot_general(
        left_rows, weight_rows, (((1,), (1,)), ((), ())), preferred_element_type=jnp.float32
    )


def thirds(scale):
    high = lax.reduce_precision(scale, 8, 7)
    rest = scale - high
    middle = lax.reduce_precision(rest, 8, 7)
    return [piece.astype(jnp.bfloat16) for piece in (high, middle, rest - middle)]


def make_body(reps, shards, cores):
    def over_rep(value):
        return lax.ppermute(value, "rep", [(i, (i + 1) % reps) for i in range(reps)])

    def over_pair(value):
        return lax.ppermute(value, "fs", [(i, i ^ 1) for i in range(shards)])

    def over_cores(value):
        return lax.ppermute(value, "tp", [(0, 1), (1, 0)])

    def sum_cores(value):
        if cores == 2:
            core = lax.axis_index("tp")
            rows = value.shape[0] // 2
            other = lax.dynamic_slice_in_dim(value, (1 - core) * rows, rows, 0)
            own = lax.dynamic_slice_in_dim(value, core * rows, rows, 0)
            other = lax.ppermute(other.astype(jnp.bfloat16), "tp", [(0, 1), (1, 0)])
            own = lax.optimization_barrier(own.astype(jnp.bfloat16))
            return own.astype(jnp.float32) + other.astype(jnp.float32)
        total = lax.psum_scatter(
            value.astype(jnp.bfloat16), "tp", scatter_dimension=0, tiled=True
        )
        return total.astype(jnp.float32)

    def gather_cores(value):
        if cores == 2:
            core = lax.axis_index("tp")
            other = lax.ppermute(value, "tp", [(0, 1), (1, 0)])
            first = jnp.where(core == 0, value, other)
            second = jnp.where(core == 0, other, value)
            return jnp.concatenate([first, second], axis=0)
        return lax.all_gather(value, "tp", axis=0, tiled=True)

    lines = [[i for i in range(shards) if i % 2 == side] for side in range(2)]

    def body(
        tokens,
        mixer_gain,
        pool_input,
        input_scale,
        group_mix,
        group_scale,
        pool_output,
        output_scale,
        channel_gain,
        gate_weight,
        gate_scale,
        up_weight,
        up_scale,
        down_weight,
        down_scale,
    ):
        rep = lax.axis_index("rep")
        side = lax.axis_index("fs") % 2
        core = lax.axis_index("tp")
        length = tokens.shape[0]
        block_width = group_mix.shape[0]
        local_width = group_mix.shape[1]

        def arranged(own, peer):
            low = jnp.where(side == 0, own, peer)
            high = jnp.where(side == 0, peer, own)
            return low, high

        def share_of(weight, which):
            share = weight.shape[-1] // (2 * reps)
            return lax.dynamic_slice_in_dim(
                weight, (rep * 2 + which) * share, share, weight.ndim - 1
            )

        def shares(weights, which):
            return [share_of(weight, which).astype(jnp.bfloat16) for weight in weights]

        def along_line(block):
            return lax.all_gather(block, "fs", axis=0, tiled=True, axis_index_groups=lines)

        columns = jnp.stack(thirds(output_scale) + thirds(down_scale), axis=1)
        columns = jnp.pad(columns, ((0, 0), (0, 128 - columns.shape[1])))
        mixer_weights = (pool_input, pool_output)
        keep = jnp.concatenate(shares(mixer_weights, side) + [columns], axis=1)
        send = jnp.concatenate(shares(mixer_weights, 1 - side) + [columns], axis=1)
        mine = along_line(jnp.concatenate(arranged(keep, over_pair(send)), axis=0))

        channel_weights = (gate_weight, up_weight, down_weight)
        keep = jnp.concatenate(shares(channel_weights, side), axis=1)
        send = jnp.concatenate(shares(channel_weights, 1 - side), axis=1)
        low, high = arranged(keep, over_pair(send))
        width = keep.shape[1] // 3
        block = jnp.concatenate([low[:, : 2 * width], high[:, : 2 * width]], axis=0)
        block, low, high, mine = lax.optimization_barrier(
            (block, low[:, 2 * width :], high[:, 2 * width :], mine)
        )
        gate_up = along_line(block)
        down_parts = [along_line(low), along_line(high)]

        quarter = local_width // 4
        feature = mine[:, 2 * quarter : 2 * quarter + 6].astype(jnp.float32).T
        output_feature = feature[0:1] + feature[1:2] + feature[2:3]
        down_feature = feature[3:4] + feature[4:5] + feature[5:6]
        mine = mine[:, : 2 * quarter]
        by_rep = over_rep(mine)
        by_side = over_pair(mine)
        split = mine.shape[0] // 2
        by_both = jnp.concatenate([over_pair(by_rep[:split]), over_rep(by_side[split:])], axis=0)
        own_low, own_high = arranged(mine, by_side)
        peer_low, peer_high = arranged(by_rep, by_both)
        quarters = [
            jnp.where(rep == 0, own_low, peer_low),
            jnp.where(rep == 0, own_high, peer_high),
            jnp.where(rep == 0, peer_low, own_low),
            jnp.where(rep == 0, peer_high, own_high),
        ]
        input_full = jnp.concatenate([piece[:, :quarter] for piece in quarters], axis=1)
        output_full = jnp.concatenate([piece[:, quarter:] for piece in quarters], axis=1)

        normed = normed_rows(tokens.astype(jnp.float32), mixer_gain)
        pool_in = (product(normed, input_full) * input_scale).astype(jnp.bfloat16)
        places = jnp.arange(length, dtype=jnp.int32)
        window_sums = pool_in.astype(jnp.float32)
        channel_group = (
            core * local_width + jnp.arange(local_width, dtype=jnp.int32)
        ) // POOL_GROUP
        pooled_mean = jnp.zeros((length, local_width), jnp.float32)
        for group_index in range(4):
            window = 2 ** (group_index + 1)
            shift = window // 2
            window_sums = window_sums + jnp.pad(window_sums[:-shift], ((shift, 0), (0, 0)))
            counts = jnp.minimum(places + 1, window).astype(jnp.float32)
            pooled_mean = jnp.where(
                channel_group[None, :] == group_index, window_sums / counts[:, None], pooled_mean
            )
        pooled = (pooled_mean - pool_in.astype(jnp.float32)).astype(jnp.bfloat16)
        local_blocks = local_width // block_width
        mixed_raw = jnp.einsum(
            "sgc,cgd->sgd",
            pooled.reshape(length, local_blocks, block_width),
            group_mix.astype(jnp.bfloat16).reshape(block_width, local_blocks, block_width),
            preferred_element_type=jnp.float32,
        ).reshape(length, local_width)
        grouped = (mixed_raw * group_scale).astype(jnp.bfloat16)
        mixer_out = sum_cores(transposed_product(grouped, output_full) * output_feature)

        rows = length // cores
        own_tokens = lax.dynamic_slice_in_dim(tokens, core * rows, rows, 0)
        middle = (own_tokens.astype(jnp.float32) + mixer_out).astype(jnp.bfloat16)
        middle = lax.optimization_barrier(middle)
        second = normed_rows(middle.astype(jnp.float32), channel_gain)

        from_rep = over_rep(second)
        from_side = over_pair(second)
        half_rows = rows // 2
        corner = jnp.concatenate(
            [over_pair(from_rep[:half_rows]), over_rep(from_side[half_rows:])], axis=0
        )
        member_rows = jnp.concatenate([second, from_rep, from_side, corner], axis=0)
        if cores == 2:
            row_sets = [over_cores(member_rows), member_rows]
        else:
            row_sets = [lax.all_gather(member_rows, "tp", axis=0, tiled=True)]

        def activated(row_set):
            both = product(row_set, gate_up)
            gate_sum = both[:, :width] * share_of(gate_scale, side)
            up_sum = both[:, width:] * share_of(up_scale, side)
            return (jax.nn.silu(gate_sum) * up_sum).astype(jnp.bfloat16)

        hidden_sets = lax.optimization_barrier([activated(row_set) for row_set in row_sets])

        def wide(value):
            return value.astype(jnp.float32)

        def scattered(down_part, hidden_sets):
            partials = [
                transposed_product(hidden, down_part).astype(jnp.bfloat16)
                for hidden in hidden_sets
            ]
            if cores == 2:
                summed = wide(over_cores(partials[0])) + wide(partials[1])
            else:
                summed = wide(
                    lax.psum_scatter(partials[0], "tp", scatter_dimension=0, tiled=True)
                )
            partial = summed.astype(jnp.bfloat16).reshape(4, rows, -1)
            half = partial.shape[2] // 2
            left, right = partial[:, :, :half], partial[:, :, half:]
            left_two = wide(left[0::2]) + wide(over_rep(left[1::2]))
            right_two = wide(right[:2]) + wide(over_pair(right[2:]))
            left_last = wide(over_pair(left_two[1].astype(jnp.bfloat16)))
            right_last = wide(over_rep(right_two[1].astype(jnp.bfloat16)))
            total = jnp.concatenate([left_two[0] + left_last, right_two[0] + right_last], axis=1)
            return total.reshape(rows, shards // 2, -1)

        low_total = scattered(down_parts[0], hidden_sets)
        low_total, hidden_sets = lax.optimization_barrier((low_total, hidden_sets))
        high_total = scattered(down_parts[1], hidden_sets)
        total = jnp.stack([low_total, high_total], axis=2)
        total = total.reshape(rows, -1)
        own_out = (middle.astype(jnp.float32) + total * down_feature).astype(jnp.bfloat16)
        return gather_cores(own_out)

    return body


MESH = pl.DeviceIdType.MESH
LANES = 128


def remote(src, dst, send, recv, device):
    return pltpu.make_async_remote_copy(
        src_ref=src,
        dst_ref=dst,
        send_sem=send,
        recv_sem=recv,
        device_id=device,
        device_id_type=MESH,
    )


def lanes_at(start, width):
    return pl.ds(pl.multiple_of(start, LANES), width)


def layer_kernel(
    planes,
    tok_any,
    gain1,
    in_scale,
    group_scale,
    out_scale,
    gain2,
    gate_scale,
    up_scale,
    down_scale,
    group_mix,
    pool_in_any,
    pool_out_any,
    gate_any,
    up_any,
    down_any,
    out_any,
    tok,
    mix,
    scales,
    normed,
    gu,
    dn,
    gu_out,
    dn_out,
    xb,
    acc,
    hid,
    pool,
    grp,
    mix_send,
    mix_recv,
    mid,
    cs_send,
    cs_recv,
    own,
    bx_send,
    bx_recv,
    by_send,
    by_recv,
    cx_send,
    cx_recv,
    cy_send,
    cy_recv,
    keep_l,
    keep_r,
    last_l,
    last_r,
    outv,
    local_sem,
    mix_recv_sem,
    mix_up,
    mix_down,
    mix_x,
    mix_corner,
    mix_y,
    sc_recv_sem,
    sc_up,
    sc_down,
    gu_recv_sem,
    gu_up,
    gu_down,
    dn_recv_sem,
    dn_up,
    dn_down,
    y_sem,
    half_sem,
    tok_recv,
    tok_send,
    cs_sems,
    b_sems,
    c_sems,
    o_sems,
):
    f32, bf16 = jnp.float32, jnp.bfloat16
    x = lax.axis_index("rep")
    f = lax.axis_index("fs")
    c = lax.axis_index("tp")
    y = lax.rem(f, 2)
    z = lax.div(f, 2)
    shards = 2 * planes
    depth = mix.shape[2]
    quarter = mix.shape[3] // 4
    rows = mid.shape[1]
    length = tok.shape[0]
    span = gu.shape[2]
    wide = span // 2 // LANES * LANES
    narrow = span // 2 - wide
    to_x = (1 - x, f, c)
    to_y = (x, 2 * z + 1 - y, c)
    to_up = (x, f + 2, c)
    to_down = (x, f - 2, c)
    to_core = (x, f, 1 - c)
    peer = 2 * z + 1 - y
    own_q = 2 * x + y
    y_q = 2 * x + 1 - y
    x_q = 2 * (1 - x) + y
    far_q = 2 * (1 - x) + 1 - y
    sends = []

    def start(copy, cond=None):
        if cond is None:
            copy.start()
        else:
            pl.when(cond)(copy.start)
        sends.append((copy, cond))

    stage = {}
    for i, ref in enumerate((gate_any, up_any, down_any)):
        stage[i] = acc.at[pl.ds(i * depth, depth), :]
    loads = [
        pltpu.make_async_copy(pool_in_any, pool.at[pl.ds(0, depth), :], local_sem.at[0]),
        pltpu.make_async_copy(pool_out_any, pool.at[pl.ds(depth, depth), :], local_sem.at[1]),
    ]
    for i, ref in enumerate((gate_any, up_any, down_any)):
        loads.append(
            pltpu.make_async_copy(ref.at[:, lanes_at(x * span, span)], stage[i], local_sem.at[2 + i])
        )
    loads.append(pltpu.make_async_copy(tok_any, tok, local_sem.at[5]))
    for load in loads:
        load.start()

    barrier = pltpu.get_barrier_semaphore()
    for device in (to_x, to_y, to_core):
        pl.semaphore_signal(barrier, inc=1, device_id=device, device_id_type=MESH)

    @pl.when(z > 0)
    def _():
        pl.semaphore_signal(barrier, inc=1, device_id=to_down, device_id_type=MESH)

    @pl.when(z < planes - 1)
    def _():
        pl.semaphore_signal(barrier, inc=1, device_id=to_up, device_id_type=MESH)

    loads[0].wait()
    mix[0, f] = pool[0:depth, :].astype(bf16)
    loads[1].wait()
    mix[1, f] = pool[depth : 2 * depth, :].astype(bf16)
    row_of = lax.broadcasted_iota(jnp.int32, (8, depth), 0)
    scales[f] = jnp.where(row_of == 0, out_scale[...], down_scale[...])
    for d in range(shards):
        dn[d, wide + narrow :, :] = jnp.zeros((dn.shape[1] - wide - narrow, dn.shape[2]), bf16)
    pl.semaphore_wait(
        barrier, 3 + jnp.where(z > 0, 1, 0) + jnp.where(z < planes - 1, 1, 0)
    )

    def mix_at(slot, q):
        return mix.at[:, slot, :, lanes_at(q * quarter, quarter)]

    def piece(kind, slot):
        if kind == "mix":
            return mix_at(slot, own_q), mix_recv_sem.at[slot, own_q], mix_up, mix_down
        if kind == "sc":
            return scales.at[slot], sc_recv_sem.at[slot], sc_up, sc_down
        if kind in ("gu0", "gu1"):
            h = int(kind[2])
            part = gu.at[slot, pl.ds(h * (depth // 2), depth // 2), :]
            return part, gu_recv_sem.at[slot, h], gu_up.at[h], gu_down.at[h]
        part = dn.at[slot, pl.ds(0, wide + narrow), :]
        return part, dn_recv_sem.at[slot], dn_up, dn_down

    def to_z(kind, slot, up=None, down=None):
        ref, recv, up_sems, down_sems = piece(kind, slot)
        if up is not None:
            start(remote(ref, ref, up_sems.at[slot], recv, to_up), up)
        if down is not None:
            start(remote(ref, ref, down_sems.at[slot], recv, to_down), down)

    def wait_piece(kind, slot, cond=None):
        ref, recv, _, _ = piece(kind, slot)
        copy = remote(ref, ref, local_sem.at[6], recv, to_x)
        if cond is None:
            copy.wait_recv()
        else:
            pl.when(cond)(copy.wait_recv)

    def own_to_z(kind, slot):
        to_z(kind, slot, z < planes - 1, z > 0)

    def hop(kind, k, t, absolute=False, then=None):
        side = t if absolute else lax.rem(y + t, 2)
        for origin, has, up, down in (
            (z - k, z >= k, jnp.logical_and(z >= k, z < planes - 1), None),
            (z + k, z + k < planes, None, jnp.logical_and(z + k < planes, z > 0)),
        ):
            slot = jnp.clip(2 * origin + side, 0, shards - 1)
            wait_piece(kind, slot, has)
            if k < planes - 1:
                to_z(kind, slot, up, down)
            if then is not None:
                then(slot, has)

    def hop_gu(k, t):
        for kind in ("gu0", "gu1"):
            hop(kind, k, t)

    mine = mix_at(f, y_q)
    start(remote(mine, mine, mix_y.at[f, y_q], mix_recv_sem.at[f, y_q], to_y))
    own_to_z("mix", f)
    start(remote(scales.at[f], scales.at[f], y_sem.at[0], sc_recv_sem.at[f], to_y))
    own_to_z("sc", f)

    lane = lax.broadcasted_iota(jnp.int32, (depth, LANES), 1)

    def join(gate_tile, up_tile, side):
        shape = gate_tile.shape
        low_lane = lax.broadcasted_iota(jnp.int32, shape, 1) < narrow
        low = jnp.where(low_lane, gate_tile, pltpu.roll(up_tile, narrow, axis=1))
        high = jnp.where(low_lane, pltpu.roll(gate_tile, narrow, axis=1), up_tile)
        return jnp.where(side == 0, low, high)

    shift_of = wide + LANES

    def build_gu(side, write):
        write(0, wide, stage[0][:, lanes_at(side * shift_of, wide)].astype(bf16))
        write(wide, wide, stage[1][:, lanes_at(side * shift_of, wide)].astype(bf16))
        tile = join(stage[0][:, wide : wide + LANES], stage[1][:, wide : wide + LANES], side)
        write(2 * wide, LANES, tile.astype(bf16))

    def build_dn(side, write):
        for j in range(wide // LANES):
            tile = stage[2][:, lanes_at(side * shift_of + j * LANES, LANES)]
            write(j * LANES, LANES, tile.T.astype(bf16))
        tile = stage[2][:, wide : wide + LANES].T
        write(wide, narrow, jnp.where(side == 0, tile[:narrow], tile[narrow:]).astype(bf16))

    def write_gu_out(at, size, value):
        gu_out[:, at : at + size] = value

    def write_gu_own(at, size, value):
        gu[f, :, at : at + size] = value

    def write_dn_out(at, size, value):
        dn_out[at : at + size, :] = value

    def write_dn_own(at, size, value):
        dn[f, at : at + size, :] = value

    loads[2].wait()
    loads[3].wait()
    build_gu(1 - y, write_gu_out)
    wait_piece("mix", peer)
    own_to_z("mix", peer)
    for h in range(2):
        part = pl.ds(h * (depth // 2), depth // 2)
        there = gu.at[f, part, :]
        start(remote(gu_out.at[part, :], there, y_sem.at[1 + h], gu_recv_sem.at[f, h], to_y))
    wait_piece("sc", peer)
    own_to_z("sc", peer)

    def spread(slot, has):
        ref = mix_at(slot, own_q)
        start(remote(ref, ref, mix_x.at[slot], mix_recv_sem.at[slot, own_q], to_x), has)
        start(remote(ref, ref, mix_y.at[slot, own_q], mix_recv_sem.at[slot, own_q], to_y), has)

    build_gu(y, write_gu_own)
    own_to_z("gu0", f)
    for t in range(2):
        hop("mix", 1, t, then=spread)
        hop("sc", 1, t)

    loads[5].wait()
    step_rows = 32

    @pl.loop(0, length // step_rows)
    def _(i):
        at = pl.ds(pl.multiple_of(i * step_rows, step_rows), step_rows)
        floats = tok[at, :].astype(f32)
        scaled = floats * lax.rsqrt(jnp.mean(floats * floats, axis=-1, keepdims=True) + epsilon)
        value = (scaled * gain1[...]).astype(bf16)
        for d in range(shards):
            normed[d, at, :] = value[:, d * depth : (d + 1) * depth]

    for k in range(2, planes):
        for t in range(2):
            hop("mix", k, t, then=spread)
            hop("sc", k, t)
        if k == planes - 2:
            own_to_z("gu1", f)
    for q in (own_q, x_q, far_q):
        ref = mix_at(f, q)
        start(remote(ref, ref, mix_y.at[f, q], mix_recv_sem.at[f, q], to_y))

    loads[4].wait()
    build_dn(1 - y, write_dn_out)
    build_dn(y, write_dn_own)

    @pl.loop(0, acc.shape[0] // 32)
    def _(r):
        acc[pl.ds(pl.multiple_of(r * 32, 32), 32), :] = jnp.zeros((32, span), f32)

    start(remote(dn_out, dn.at[f, pl.ds(0, wide + narrow), :], y_sem.at[3], dn_recv_sem.at[f], to_y))

    def wait_mix(slot, q, cond=None):
        ref = mix_at(slot, q)
        copy = remote(ref, ref, local_sem.at[6], mix_recv_sem.at[slot, q], to_x)
        if cond is None:
            copy.wait_recv()
        else:
            pl.when(cond)(copy.wait_recv)

    def others(k, t, do):
        for origin, has in ((z - k, z >= k), (z + k, z + k < planes)):
            do(jnp.clip(2 * origin + lax.rem(y + t, 2), 0, shards - 1), has)

    def corner(slot, has):
        wait_mix(slot, y_q, has)
        ref = mix_at(slot, y_q)
        start(remote(ref, ref, mix_corner.at[slot], mix_recv_sem.at[slot, y_q], to_x), has)

    def rest(slot, has):
        wait_mix(slot, x_q, has)
        wait_mix(slot, far_q, has)

    for kind in ("gu0", "gu1"):
        wait_piece(kind, peer)
        own_to_z(kind, peer)
    for k in range(1, planes):
        for t in range(2):
            others(k, 1 - t, corner)
    hop_gu(1, 0)
    for k in range(1, planes):
        for t in range(2):
            others(k, t, rest)
    for q in (y_q, x_q, far_q):
        wait_mix(peer, q)

    pool[...] = jnp.zeros(pool.shape, f32)

    @pl.loop(0, shards)
    def _(d):
        pool[...] += jnp.dot(normed[d], mix[0, d], preferred_element_type=f32)

    local_width = pool.shape[1]
    place = lax.broadcasted_iota(jnp.int32, (length, LANES), 0)
    for q in range(local_width // LANES):
        at = slice(q * LANES, (q + 1) * LANES)
        value = (pool[:, at] * in_scale[:, at]).astype(bf16).astype(f32)
        group = lax.div(c * local_width + q * LANES, POOL_GROUP)
        sums = value
        mean = jnp.zeros_like(value)
        for index in range(4):
            window = 2 ** (index + 1)
            shift = window // 2
            sums = sums + jnp.where(place >= shift, pltpu.roll(sums, shift, axis=0), 0.0)
            counts = jnp.minimum(place + 1, window).astype(f32)
            mean = jnp.where(group == index, sums / counts, mean)
        pooled = (mean - value).astype(bf16)
        mixed = jnp.dot(pooled, group_mix[:, at].astype(bf16), preferred_element_type=f32)
        grp[:, at] = (mixed * group_scale[:, at]).astype(bf16)

    def mixer_rows(d, core):
        left = grp[pl.ds(pl.multiple_of(core * rows, rows), rows), :]
        value = lax.dot_general(
            left, mix[1, d], (((1,), (1,)), ((), ())), preferred_element_type=f32
        )
        return (value * scales[d, 0:1, :]).astype(bf16)

    @pl.loop(0, shards)
    def _(d):
        mix_send[d] = mixer_rows(d, 1 - c)

    start(remote(mix_send, mix_recv, half_sem.at[0], half_sem.at[1], to_core))
    hop_gu(1, 1)

    @pl.loop(0, shards)
    def _(d):
        mid[d] = mixer_rows(d, c)

    remote(mix_send, mix_recv, half_sem.at[0], half_sem.at[1], to_core).wait_recv()
    my_rows = pl.ds(pl.multiple_of(c * rows, rows), rows)
    block = 2 * (2 * x + y) + c
    for part in range(4):
        size = rows // 4
        at = pl.ds(part * size, size)
        tok_at = pl.ds(pl.multiple_of(c * rows + part * size, size), size)
        squares = jnp.zeros((size, depth), f32)
        for d in range(shards):
            value = (
                tok[tok_at, d * depth : (d + 1) * depth].astype(f32)
                + (mid[d, at, :].astype(f32) + mix_recv[d, at, :].astype(f32))
            ).astype(bf16)
            mid[d, at, :] = value
            wide_value = value.astype(f32)
            squares = squares + wide_value * wide_value
        mean = jnp.sum(squares, axis=-1, keepdims=True) / (shards * depth)
        factor = lax.rsqrt(mean + epsilon)
        to_at = pl.ds(pl.multiple_of(block * rows + part * size, size), size)
        for d in range(shards):
            scaled = mid[d, at, :].astype(f32) * factor
            gain = gain2[:, d * depth : (d + 1) * depth]
            xb[d, to_at, :] = (scaled * gain).astype(bf16)

    half = rows // 2

    def rows_of(core, bx, by, h=None):
        first = (2 * (2 * bx + by) + core) * rows
        if h is None:
            return xb.at[:, pl.ds(pl.multiple_of(first, rows), rows), :]
        return xb.at[:, pl.ds(pl.multiple_of(first + h * half, half), half), :]

    def send_rows(ref, i, j, device):
        start(remote(ref, ref, tok_send.at[i], tok_recv.at[j], device))

    def wait_rows(ref, j):
        remote(ref, ref, local_sem.at[6], tok_recv.at[j], to_x).wait_recv()

    own_group = own_q

    orders = []
    for plane in range(planes):
        near = sorted(range(planes), key=lambda p: (abs(p - plane), p))
        orders.append(near)

    def plane_at(j):
        value = jnp.int32(0)
        for plane in range(planes):
            for i in range(planes):
                here = jnp.logical_and(z == plane, j == i)
                value = jnp.where(here, orders[plane][i], value)
        return value

    def unit(group, j):
        at = pl.ds(pl.multiple_of(group * 2 * rows, 2 * rows), 2 * rows)
        slot = 2 * plane_at(j)
        value = jnp.dot(xb[slot, at, :], gu[slot], preferred_element_type=f32)
        value += jnp.dot(xb[slot + 1, at, :], gu[slot + 1], preferred_element_type=f32)
        acc[at, :] += value

    for h in range(2):
        send_rows(rows_of(c, x, y, h), h, h, to_x)
        send_rows(rows_of(c, x, y, 1 - h), 2 + h, 2 + 1 - h, to_y)
    send_rows(rows_of(c, x, y), 4, 6, to_core)
    wait_rows(rows_of(1 - c, x, y), 6)

    @pl.loop(0, 2)
    def _(j):
        unit(own_group, j)

    hop_gu(2, 0)
    wait_rows(rows_of(c, 1 - x, y, 0), 0)
    send_rows(rows_of(c, 1 - x, y, 0), 5, 4, to_y)
    wait_rows(rows_of(c, x, 1 - y, 1), 3)
    send_rows(rows_of(c, x, 1 - y, 1), 6, 5, to_x)
    wait_rows(rows_of(c, 1 - x, y, 1), 1)
    send_rows(rows_of(c, 1 - x, y), 7, 7, to_core)
    wait_rows(rows_of(c, x, 1 - y, 0), 2)
    send_rows(rows_of(c, x, 1 - y), 8, 8, to_core)
    hop_gu(2, 1)
    wait_piece("dn", peer)
    own_to_z("dn", 2 * z)
    own_to_z("dn", 2 * z + 1)
    all_rows = xb.shape[1]
    tall = 512
    unit(own_group, 2)
    wait_rows(rows_of(1 - c, 1 - x, y), 7)
    wait_rows(rows_of(1 - c, x, 1 - y), 8)

    @pl.loop(0, 2)
    def _(g):
        group = jnp.where(g == 0, x_q, y_q)

        @pl.loop(0, planes - 1)
        def _(j):
            unit(group, j)

    wait_rows(rows_of(c, 1 - x, 1 - y, 0), 4)
    wait_rows(rows_of(c, 1 - x, 1 - y, 1), 5)
    send_rows(rows_of(c, 1 - x, 1 - y), 9, 9, to_core)
    wait_rows(rows_of(1 - c, 1 - x, 1 - y), 9)

    @pl.loop(0, planes - 1)
    def _(j):
        unit(far_q, j)

    for t in range(2):
        hop_gu(planes - 1, t)

        @pl.loop(0, 4)
        def _(g):
            at = pl.ds(pl.multiple_of(g * 2 * rows, 2 * rows), 2 * rows)
            slot = 2 * plane_at(planes - 1) + lax.rem(y + t, 2)
            acc[at, :] += jnp.dot(xb[slot, at, :], gu[slot], preferred_element_type=f32)

    wide_tiles = wide // LANES
    first_row = x * (span // LANES)
    joint_row = pl.ds(first_row + wide_tiles, 1)
    joint_scale = join(
        jnp.broadcast_to(gate_scale[joint_row, :], (8, LANES)),
        jnp.broadcast_to(up_scale[joint_row, :], (8, LANES)),
        y,
    )[0:1]
    gate_rows, up_rows = [], []
    for j in range(wide_tiles):
        at = pl.ds(first_row + y * (wide_tiles + 1) + j, 1)
        gate_rows.append(gate_scale[at, :])
        up_rows.append(up_scale[at, :])
    act = 64

    @pl.loop(0, all_rows // act)
    def _(r):
        at = pl.ds(pl.multiple_of(r * act, act), act)
        group = lax.div(r * act, 2 * rows)
        core = lax.rem(lax.div(r * act, rows), 2)
        inside = lax.rem(r * act, rows)
        to = pl.ds(pl.multiple_of(core * 4 * rows + group * rows + inside, act), act)
        for j in range(wide_tiles):
            cols = slice(j * LANES, (j + 1) * LANES)
            gate = acc[at, cols] * gate_rows[j]
            up = acc[at, wide + j * LANES : wide + (j + 1) * LANES] * up_rows[j]
            hid[to, cols] = (gate / (1.0 + jnp.exp(-gate)) * up).astype(bf16)
        both = acc[at, 2 * wide :] * joint_scale
        value = both / (1.0 + jnp.exp(-both)) * pltpu.roll(both, narrow, axis=1)
        keep = lax.broadcasted_iota(jnp.int32, (act, LANES), 1) < narrow
        hid[to, wide:] = jnp.where(keep, value, 0.0).astype(bf16)

    core_rows = all_rows // 2
    two = 2 * rows
    low, high = slice(0, LANES), slice(LANES, 2 * LANES)

    def slot_at(i):
        return 2 * plane_at(i // 2) + i % 2

    def cs_copy(i):
        s = i % 2
        return remote(cs_send.at[s], cs_recv.at[i], cs_sems.at[s], cs_sems.at[2 + i], to_core)

    def bx_copy(i):
        s = i % 2
        return remote(bx_send.at[s], bx_recv.at[i], b_sems.at[0, s], b_sems.at[0, 2 + i], to_x)

    def by_copy(i):
        s = i % 2
        return remote(by_send.at[s], by_recv.at[i], b_sems.at[1, s], b_sems.at[1, 2 + i], to_y)

    def cx_copy(i):
        s = i % 2
        return remote(cx_send.at[s], cx_recv.at[i], c_sems.at[0, s], c_sems.at[0, 2 + i], to_x)

    def cy_copy(i):
        s = i % 2
        return remote(cy_send.at[s], cy_recv.at[i], c_sems.at[1, s], c_sems.at[1, 2 + i], to_y)

    def out_at(i, core):
        d = slot_at(i)
        return out_any.at[pl.ds(pl.multiple_of(core * rows, rows), rows), lanes_at(d * depth, depth)]

    def out_local(i):
        return pltpu.make_async_copy(outv.at[i], out_at(i, c), o_sems.at[0, i])

    def out_remote(i):
        return remote(outv.at[i], out_at(i, c), o_sems.at[1, i], o_sems.at[2, i], to_core)

    def first_stage(i):
        slot = slot_at(i)
        s = i % 2
        if i >= 2:
            cs_copy(i - 2).wait_send()
        weight = dn[slot]

        @pl.loop(0, core_rows // tall)
        def _(r):
            at = pl.ds(pl.multiple_of(r * tall, tall), tall)
            there = pl.ds(pl.multiple_of((1 - c) * core_rows + r * tall, tall), tall)
            cs_send[s, at, :] = jnp.dot(hid[there, :], dn[slot], preferred_element_type=f32).astype(bf16)

        cs_copy(i).start()

        @pl.loop(0, core_rows // tall)
        def _(r):
            at = pl.ds(pl.multiple_of(r * tall, tall), tall)
            here = pl.ds(pl.multiple_of(c * core_rows + r * tall, tall), tall)
            own[at, :] = jnp.dot(hid[here, :], dn[slot], preferred_element_type=f32)

    def block_rows(bx, by):
        return pl.ds(pl.multiple_of((2 * bx + by) * rows, rows), rows)

    def second_stage(i):
        s = i % 2
        cs_copy(i).wait_recv()
        if i >= 2:
            bx_copy(i - 2).wait_send()
            by_copy(i - 2).wait_send()
        for b in range(2):
            at = block_rows(1 - x, b)
            value = own[at, low] + cs_recv[i, at, low].astype(f32)
            bx_send[s, b] = value.astype(bf16)
        bx_copy(i).start()
        for b in range(2):
            at = block_rows(b, 1 - y)
            value = own[at, high] + cs_recv[i, at, high].astype(f32)
            by_send[s, b] = value.astype(bf16)
        by_copy(i).start()
        for b in range(2):
            at = block_rows(x, b)
            keep_l[s, b] = own[at, low] + cs_recv[i, at, low].astype(f32)
            at = block_rows(b, y)
            keep_r[s, b] = own[at, high] + cs_recv[i, at, high].astype(f32)

    def third_stage(i):
        s = i % 2
        if i >= 2:
            cx_copy(i - 2).wait_send()
            cy_copy(i - 2).wait_send()
        bx_copy(i).wait_recv()
        cy_send[s] = (keep_l[s, 1 - y] + bx_recv[i, 1 - y].astype(f32)).astype(bf16)
        cy_copy(i).start()
        by_copy(i).wait_recv()
        cx_send[s] = (keep_r[s, 1 - x] + by_recv[i, 1 - x].astype(f32)).astype(bf16)
        cx_copy(i).start()
        last_l[s] = keep_l[s, y] + bx_recv[i, y].astype(f32)
        last_r[s] = keep_r[s, x] + by_recv[i, x].astype(f32)

    def fourth_stage(i):
        s = i % 2
        d = slot_at(i)
        scale = scales[d, 1:2, :]
        cy_copy(i).wait_recv()
        total = last_l[s] + cy_recv[i].astype(f32)
        outv[i, :, low] = (mid[d, :, low].astype(f32) + total * scale[:, low]).astype(bf16)
        cx_copy(i).wait_recv()
        total = last_r[s] + cx_recv[i].astype(f32)
        outv[i, :, high] = (mid[d, :, high].astype(f32) + total * scale[:, high]).astype(bf16)
        out_remote(i).start()
        out_local(i).start()

    stages = {1: first_stage, 2: second_stage, 3: third_stage, 4: fourth_stage}
    done = set()

    def run(stage, i):
        if i < 0 or i >= shards or (stage, i) in done:
            return
        done.add((stage, i))
        stages[stage](i)

    for i in range(shards):
        if i >= shards - 2:
            run(4, i - 4)
            run(4, i - 3)
            if i == shards - 1:
                run(4, i - 2)
                run(3, i - 1)
            else:
                run(3, i - 2)
        if i >= 2:
            hop("dn", i // 2, i % 2, absolute=True)
        run(1, i)
        run(4, i - 4)
        run(3, i - 2)
        run(2, i)
        if i == shards - 2:
            run(4, i - 3)
            run(3, i - 1)
    run(4, shards - 2)
    run(3, shards - 1)
    run(4, shards - 1)

    for copy, cond in sends:
        if cond is None:
            copy.wait_send()
        else:
            pl.when(cond)(copy.wait_send)
    for i in (shards - 2, shards - 1):
        for make in (cs_copy, bx_copy, by_copy, cx_copy, cy_copy):
            make(i).wait_send()
    for i in range(shards):
        out_local(i).wait()
        out_remote(i).wait_send()
        remote(outv.at[i], out_at(i, 1 - c), o_sems.at[1, i], o_sems.at[2, i], to_core).wait_recv()


def make_fast(shards):
    planes = shards // 2

    def body(
        tokens,
        mixer_gain,
        pool_input,
        input_scale,
        group_mix,
        group_scale,
        pool_output,
        output_scale,
        channel_gain,
        gate_weight,
        gate_scale,
        up_weight,
        up_scale,
        down_weight,
        down_scale,
    ):
        f32, bf16 = jnp.float32, jnp.bfloat16
        length, width = tokens.shape
        depth, local_width = pool_input.shape
        span = gate_weight.shape[1] // 2
        padded = (span // 2 + LANES - 1) // LANES * LANES
        rows = length // 2
        everything = 8 * rows
        vmem = pl.BlockSpec(memory_space=pltpu.VMEM)
        anywhere = pl.BlockSpec(memory_space=pl.ANY)
        dma = pltpu.SemaphoreType.DMA
        scratch = [
            pltpu.VMEM((length, width), bf16),
            pltpu.VMEM((2, shards, depth, local_width), bf16),
            pltpu.VMEM((shards, 8, depth), f32),
            pltpu.VMEM((shards, length, depth), bf16),
            pltpu.VMEM((shards, depth, span), bf16),
            pltpu.VMEM((shards, padded, depth), bf16),
            pltpu.VMEM((depth, span), bf16),
            pltpu.VMEM((span // 2, depth), bf16),
            pltpu.VMEM((shards, everything, depth), bf16),
            pltpu.VMEM((everything, span), f32),
            pltpu.VMEM((everything, padded), bf16),
            pltpu.VMEM((length, local_width), f32),
            pltpu.VMEM((length, local_width), bf16),
            pltpu.VMEM((shards, rows, depth), bf16),
            pltpu.VMEM((shards, rows, depth), bf16),
            pltpu.VMEM((shards, rows, depth), bf16),
            pltpu.VMEM((2, 4 * rows, depth), bf16),
            pltpu.VMEM((shards, 4 * rows, depth), bf16),
            pltpu.VMEM((4 * rows, depth), f32),
            pltpu.VMEM((2, 2, rows, LANES), bf16),
            pltpu.VMEM((shards, 2, rows, LANES), bf16),
            pltpu.VMEM((2, 2, rows, LANES), bf16),
            pltpu.VMEM((shards, 2, rows, LANES), bf16),
            pltpu.VMEM((2, rows, LANES), bf16),
            pltpu.VMEM((shards, rows, LANES), bf16),
            pltpu.VMEM((2, rows, LANES), bf16),
            pltpu.VMEM((shards, rows, LANES), bf16),
            pltpu.VMEM((2, 2, rows, LANES), f32),
            pltpu.VMEM((2, 2, rows, LANES), f32),
            pltpu.VMEM((2, rows, LANES), f32),
            pltpu.VMEM((2, rows, LANES), f32),
            pltpu.VMEM((shards, rows, depth), bf16),
            dma((7,)),
            dma((shards, 4)),
            dma((shards,)),
            dma((shards,)),
            dma((shards,)),
            dma((shards,)),
            dma((shards, 4)),
            dma((shards,)),
            dma((shards,)),
            dma((shards,)),
            dma((shards, 2)),
            dma((2, shards)),
            dma((2, shards)),
            dma((shards,)),
            dma((shards,)),
            dma((shards,)),
            dma((4,)),
            dma((2,)),
            dma((10,)),
            dma((10,)),
            dma((2 + shards,)),
            dma((2, 2 + shards)),
            dma((2, 2 + shards)),
            dma((3, shards)),
        ]
        row = lambda value: value.reshape(1, -1)
        return pl.pallas_call(
            functools.partial(layer_kernel, planes),
            name="layer",
            out_shape=jax.ShapeDtypeStruct((length, width), bf16),
            in_specs=[anywhere] + [vmem] * 9 + [anywhere] * 5,
            out_specs=anywhere,
            scratch_shapes=scratch,
            compiler_params=pltpu.CompilerParams(
                collective_id=0, has_side_effects=True, vmem_limit_bytes=67043328
            ),
        )(
            tokens,
            row(mixer_gain),
            row(input_scale),
            row(group_scale),
            row(output_scale),
            row(channel_gain),
            gate_scale.reshape(-1, LANES),
            up_scale.reshape(-1, LANES),
            row(down_scale),
            group_mix,
            pool_input,
            pool_output,
            gate_weight,
            up_weight,
            down_weight,
        )

    return body


def solution(mesh):
    in_specs = (
        P(("rep", "fs"), None),
        P(),
        P("fs", "tp"),
        P("tp"),
        P(None, "tp"),
        P("tp"),
        P("fs", "tp"),
        P("fs"),
        P(),
        P("fs", "tp"),
        P("tp"),
        P("fs", "tp"),
        P("tp"),
        P("fs", "tp"),
        P("fs"),
    )
    out_specs = P(("rep", "fs"), None)
    reps, shards, cores = mesh.shape["rep"], mesh.shape["fs"], mesh.shape["tp"]
    fast = reps == 2 and cores == 2 and shards % 2 == 0
    body = make_fast(shards) if fast else make_body(reps, shards, cores)
    return jax.shard_map(body, mesh=mesh, in_specs=in_specs, out_specs=out_specs, check_vma=False)
```

```python
import functools

import jax
import jax.numpy as jnp
from jax import lax
from jax.experimental import pallas as pl
from jax.experimental.pallas import tpu as pltpu
from jax.sharding import PartitionSpec as P

POOL_GROUP = 256

epsilon = 1e-06


def normed_rows(floats, gain_row):
    scaled = floats * lax.rsqrt(jnp.mean(floats * floats, axis=-1, keepdims=True) + epsilon)
    return (scaled * gain_row).astype(jnp.bfloat16)


def product(left_rows, weight):
    return jnp.dot(left_rows, weight, preferred_element_type=jnp.float32)


def transposed_product(left_rows, weight_rows):
    return lax.dot_general(
        left_rows, weight_rows, (((1,), (1,)), ((), ())), preferred_element_type=jnp.float32
    )


def thirds(scale):
    high = lax.reduce_precision(scale, 8, 7)
    rest = scale - high
    middle = lax.reduce_precision(rest, 8, 7)
    return [piece.astype(jnp.bfloat16) for piece in (high, middle, rest - middle)]


def make_body(reps, shards, cores):
    def over_rep(value):
        return lax.ppermute(value, "rep", [(i, (i + 1) % reps) for i in range(reps)])

    def over_pair(value):
        return lax.ppermute(value, "fs", [(i, i ^ 1) for i in range(shards)])

    def over_cores(value):
        return lax.ppermute(value, "tp", [(0, 1), (1, 0)])

    def sum_cores(value):
        if cores == 2:
            core = lax.axis_index("tp")
            rows = value.shape[0] // 2
            other = lax.dynamic_slice_in_dim(value, (1 - core) * rows, rows, 0)
            own = lax.dynamic_slice_in_dim(value, core * rows, rows, 0)
            other = lax.ppermute(other.astype(jnp.bfloat16), "tp", [(0, 1), (1, 0)])
            own = lax.optimization_barrier(own.astype(jnp.bfloat16))
            return own.astype(jnp.float32) + other.astype(jnp.float32)
        total = lax.psum_scatter(
            value.astype(jnp.bfloat16), "tp", scatter_dimension=0, tiled=True
        )
        return total.astype(jnp.float32)

    def gather_cores(value):
        if cores == 2:
            core = lax.axis_index("tp")
            other = lax.ppermute(value, "tp", [(0, 1), (1, 0)])
            first = jnp.where(core == 0, value, other)
            second = jnp.where(core == 0, other, value)
            return jnp.concatenate([first, second], axis=0)
        return lax.all_gather(value, "tp", axis=0, tiled=True)

    lines = [[i for i in range(shards) if i % 2 == side] for side in range(2)]

    def body(
        tokens,
        mixer_gain,
        pool_input,
        input_scale,
        group_mix,
        group_scale,
        pool_output,
        output_scale,
        channel_gain,
        gate_weight,
        gate_scale,
        up_weight,
        up_scale,
        down_weight,
        down_scale,
    ):
        rep = lax.axis_index("rep")
        side = lax.axis_index("fs") % 2
        core = lax.axis_index("tp")
        length = tokens.shape[0]
        block_width = group_mix.shape[0]
        local_width = group_mix.shape[1]

        def arranged(own, peer):
            low = jnp.where(side == 0, own, peer)
            high = jnp.where(side == 0, peer, own)
            return low, high

        def share_of(weight, which):
            share = weight.shape[-1] // (2 * reps)
            return lax.dynamic_slice_in_dim(
                weight, (rep * 2 + which) * share, share, weight.ndim - 1
            )

        def shares(weights, which):
            return [share_of(weight, which).astype(jnp.bfloat16) for weight in weights]

        def along_line(block):
            return lax.all_gather(block, "fs", axis=0, tiled=True, axis_index_groups=lines)

        columns = jnp.stack(thirds(output_scale) + thirds(down_scale), axis=1)
        columns = jnp.pad(columns, ((0, 0), (0, 128 - columns.shape[1])))
        mixer_weights = (pool_input, pool_output)
        keep = jnp.concatenate(shares(mixer_weights, side) + [columns], axis=1)
        send = jnp.concatenate(shares(mixer_weights, 1 - side) + [columns], axis=1)
        mine = along_line(jnp.concatenate(arranged(keep, over_pair(send)), axis=0))

        channel_weights = (gate_weight, up_weight, down_weight)
        keep = jnp.concatenate(shares(channel_weights, side), axis=1)
        send = jnp.concatenate(shares(channel_weights, 1 - side), axis=1)
        low, high = arranged(keep, over_pair(send))
        width = keep.shape[1] // 3
        block = jnp.concatenate([low[:, : 2 * width], high[:, : 2 * width]], axis=0)
        block, low, high, mine = lax.optimization_barrier(
            (block, low[:, 2 * width :], high[:, 2 * width :], mine)
        )
        gate_up = along_line(block)
        down_parts = [along_line(low), along_line(high)]

        quarter = local_width // 4
        feature = mine[:, 2 * quarter : 2 * quarter + 6].astype(jnp.float32).T
        output_feature = feature[0:1] + feature[1:2] + feature[2:3]
        down_feature = feature[3:4] + feature[4:5] + feature[5:6]
        mine = mine[:, : 2 * quarter]
        by_rep = over_rep(mine)
        by_side = over_pair(mine)
        split = mine.shape[0] // 2
        by_both = jnp.concatenate([over_pair(by_rep[:split]), over_rep(by_side[split:])], axis=0)
        own_low, own_high = arranged(mine, by_side)
        peer_low, peer_high = arranged(by_rep, by_both)
        quarters = [
            jnp.where(rep == 0, own_low, peer_low),
            jnp.where(rep == 0, own_high, peer_high),
            jnp.where(rep == 0, peer_low, own_low),
            jnp.where(rep == 0, peer_high, own_high),
        ]
        input_full = jnp.concatenate([piece[:, :quarter] for piece in quarters], axis=1)
        output_full = jnp.concatenate([piece[:, quarter:] for piece in quarters], axis=1)

        normed = normed_rows(tokens.astype(jnp.float32), mixer_gain)
        pool_in = (product(normed, input_full) * input_scale).astype(jnp.bfloat16)
        places = jnp.arange(length, dtype=jnp.int32)
        window_sums = pool_in.astype(jnp.float32)
        channel_group = (
            core * local_width + jnp.arange(local_width, dtype=jnp.int32)
        ) // POOL_GROUP
        pooled_mean = jnp.zeros((length, local_width), jnp.float32)
        for group_index in range(4):
            window = 2 ** (group_index + 1)
            shift = window // 2
            window_sums = window_sums + jnp.pad(window_sums[:-shift], ((shift, 0), (0, 0)))
            counts = jnp.minimum(places + 1, window).astype(jnp.float32)
            pooled_mean = jnp.where(
                channel_group[None, :] == group_index, window_sums / counts[:, None], pooled_mean
            )
        pooled = (pooled_mean - pool_in.astype(jnp.float32)).astype(jnp.bfloat16)
        local_blocks = local_width // block_width
        mixed_raw = jnp.einsum(
            "sgc,cgd->sgd",
            pooled.reshape(length, local_blocks, block_width),
            group_mix.astype(jnp.bfloat16).reshape(block_width, local_blocks, block_width),
            preferred_element_type=jnp.float32,
        ).reshape(length, local_width)
        grouped = (mixed_raw * group_scale).astype(jnp.bfloat16)
        mixer_out = sum_cores(transposed_product(grouped, output_full) * output_feature)

        rows = length // cores
        own_tokens = lax.dynamic_slice_in_dim(tokens, core * rows, rows, 0)
        middle = (own_tokens.astype(jnp.float32) + mixer_out).astype(jnp.bfloat16)
        middle = lax.optimization_barrier(middle)
        second = normed_rows(middle.astype(jnp.float32), channel_gain)

        from_rep = over_rep(second)
        from_side = over_pair(second)
        half_rows = rows // 2
        corner = jnp.concatenate(
            [over_pair(from_rep[:half_rows]), over_rep(from_side[half_rows:])], axis=0
        )
        member_rows = jnp.concatenate([second, from_rep, from_side, corner], axis=0)
        if cores == 2:
            row_sets = [over_cores(member_rows), member_rows]
        else:
            row_sets = [lax.all_gather(member_rows, "tp", axis=0, tiled=True)]

        def activated(row_set):
            both = product(row_set, gate_up)
            gate_sum = both[:, :width] * share_of(gate_scale, side)
            up_sum = both[:, width:] * share_of(up_scale, side)
            return (jax.nn.silu(gate_sum) * up_sum).astype(jnp.bfloat16)

        hidden_sets = lax.optimization_barrier([activated(row_set) for row_set in row_sets])

        def wide(value):
            return value.astype(jnp.float32)

        def scattered(down_part, hidden_sets):
            partials = [
                transposed_product(hidden, down_part).astype(jnp.bfloat16)
                for hidden in hidden_sets
            ]
            if cores == 2:
                summed = wide(over_cores(partials[0])) + wide(partials[1])
            else:
                summed = wide(
                    lax.psum_scatter(partials[0], "tp", scatter_dimension=0, tiled=True)
                )
            partial = summed.astype(jnp.bfloat16).reshape(4, rows, -1)
            half = partial.shape[2] // 2
            left, right = partial[:, :, :half], partial[:, :, half:]
            left_two = wide(left[0::2]) + wide(over_rep(left[1::2]))
            right_two = wide(right[:2]) + wide(over_pair(right[2:]))
            left_last = wide(over_pair(left_two[1].astype(jnp.bfloat16)))
            right_last = wide(over_rep(right_two[1].astype(jnp.bfloat16)))
            total = jnp.concatenate([left_two[0] + left_last, right_two[0] + right_last], axis=1)
            return total.reshape(rows, shards // 2, -1)

        low_total = scattered(down_parts[0], hidden_sets)
        low_total, hidden_sets = lax.optimization_barrier((low_total, hidden_sets))
        high_total = scattered(down_parts[1], hidden_sets)
        total = jnp.stack([low_total, high_total], axis=2)
        total = total.reshape(rows, -1)
        own_out = (middle.astype(jnp.float32) + total * down_feature).astype(jnp.bfloat16)
        return gather_cores(own_out)

    return body


MESH = pl.DeviceIdType.MESH
LANES = 128


def remote(src, dst, send, recv, device):
    return pltpu.make_async_remote_copy(
        src_ref=src,
        dst_ref=dst,
        send_sem=send,
        recv_sem=recv,
        device_id=device,
        device_id_type=MESH,
    )


def lanes_at(start, width):
    return pl.ds(pl.multiple_of(start, LANES), width)


def layer_kernel(
    planes,
    tok_any,
    gain1_any,
    in_scale_any,
    group_scale_any,
    out_scale_any,
    gain2_any,
    gate_scale_any,
    up_scale_any,
    down_scale_any,
    group_mix_any,
    pool_in_any,
    pool_out_any,
    gate_any,
    up_any,
    down_any,
    out,
    gain1,
    in_scale,
    group_scale,
    out_scale,
    gain2,
    gate_scale,
    up_scale,
    down_scale,
    group_mix,
    tok,
    mix,
    scales,
    normed,
    gu,
    dn,
    gu_out,
    dn_out,
    xb,
    acc,
    hid,
    pool,
    grp,
    mix_send,
    mix_recv,
    mid,
    cs_recv,
    bx_send,
    bx_recv,
    by_send,
    by_recv,
    cx_send,
    cx_recv,
    cy_send,
    cy_recv,
    keep_l,
    keep_r,
    last_l,
    last_r,
    recv_sem,
    mix_z,
    sc_z,
    gu_z,
    sc_recv_sem,
    gu_recv_sem,
    dn_recv_sem,
    mix_x,
    mix_corner,
    mix_y,
    y_sem,
    half_sem,
    tok_recv,
    tok_send,
):
    f32, bf16 = jnp.float32, jnp.bfloat16
    x = lax.axis_index("rep")
    f = lax.axis_index("fs")
    c = lax.axis_index("tp")
    y = lax.rem(f, 2)
    z = lax.div(f, 2)
    shards = 2 * planes
    depth = mix.shape[2]
    quarter = mix.shape[3] // 4
    rows = mid.shape[1]
    length = tok.shape[0]
    span = gu.shape[2]
    wide = span // 2 // LANES * LANES
    narrow = span // 2 - wide
    to_x = (1 - x, f, c)
    to_y = (x, 2 * z + 1 - y, c)
    to_up = (x, f + 2, c)
    to_down = (x, f - 2, c)
    to_core = (x, f, 1 - c)
    peer = 2 * z + 1 - y
    own_q = 2 * x + y
    y_q = 2 * x + 1 - y
    x_q = 2 * (1 - x) + y
    far_q = 2 * (1 - x) + 1 - y
    sends = []

    def start(copy, cond=None, group="mix"):
        if cond is None:
            copy.start()
        else:
            pl.when(cond)(copy.start)
        sends.append((copy, cond, group))

    def settle(which):
        for copy, cond, group in sends:
            if group == which and cond is None:
                copy.wait_send()
            elif group == which:
                pl.when(cond)(copy.wait_send)

    stage = {}
    for i, ref in enumerate((gate_any, up_any, down_any)):
        stage[i] = acc.at[pl.ds(i * depth, depth), :]
    loads = [
        pltpu.make_async_copy(pool_in_any, pool.at[pl.ds(0, depth), :], recv_sem.at[4 * shards]),
        pltpu.make_async_copy(pool_out_any, pool.at[pl.ds(depth, depth), :], recv_sem.at[4 * shards + 1]),
    ]
    for i, ref in enumerate((gate_any, up_any, down_any)):
        loads.append(
            pltpu.make_async_copy(
                ref.at[:, lanes_at(x * span, span)], stage[i], recv_sem.at[4 * shards + 2 + i]
            )
        )
    loads.append(pltpu.make_async_copy(tok_any, tok, recv_sem.at[4 * shards + 5]))
    small = []
    for i, (source, target) in enumerate(
        (
            (out_scale_any, out_scale),
            (down_scale_any, down_scale),
            (gain1_any, gain1),
            (in_scale_any, in_scale),
            (group_scale_any, group_scale),
            (group_mix_any, group_mix),
            (gain2_any, gain2),
            (gate_scale_any, gate_scale),
            (up_scale_any, up_scale),
        )
    ):
        small.append(pltpu.make_async_copy(source, target, recv_sem.at[4 * shards + 6 + i]))
    for load in loads[:2] + small[:2] + loads[2:4] + small[2:] + loads[4:]:
        load.start()

    barrier = pltpu.get_barrier_semaphore()
    for device in (to_x, to_y, to_core):
        pl.semaphore_signal(barrier, inc=1, device_id=device, device_id_type=MESH)

    @pl.when(z > 0)
    def _():
        pl.semaphore_signal(barrier, inc=1, device_id=to_down, device_id_type=MESH)

    @pl.when(z < planes - 1)
    def _():
        pl.semaphore_signal(barrier, inc=1, device_id=to_up, device_id_type=MESH)

    loads[0].wait()
    mix[0, f] = pool[0:depth, :].astype(bf16)
    loads[1].wait()
    mix[1, f] = pool[depth : 2 * depth, :].astype(bf16)
    small[0].wait()
    scales[f, 0:1, :] = out_scale[...]
    small[1].wait()
    scales[f, 1:2, :] = down_scale[...]
    for d in range(shards):
        dn[d, wide + narrow :, :] = jnp.zeros((dn.shape[1] - wide - narrow, dn.shape[2]), bf16)
    pl.semaphore_wait(
        barrier, 3 + jnp.where(z > 0, 1, 0) + jnp.where(z < planes - 1, 1, 0)
    )

    def mix_recv_at(slot, q):
        return recv_sem.at[4 * slot + q]

    def mix_at(slot, q):
        return mix.at[:, slot, :, lanes_at(q * quarter, quarter)]

    def piece(kind, slot):
        if kind == "mix":
            return mix_at(slot, own_q), mix_recv_at(slot, own_q), mix_z
        if kind == "sc":
            return scales.at[slot], sc_recv_sem.at[slot], sc_z
        if kind in ("gu0", "gu1"):
            h = int(kind[2])
            part = gu.at[slot, pl.ds(h * (depth // 2), depth // 2), :]
            return part, gu_recv_sem.at[h, slot], gu_z.at[h]
        if kind == "dn":
            part, h = dn.at[slot, pl.ds(0, wide + narrow), :], 0
        else:
            h = ("dna", "dnb").index(kind)
            lanes = pl.ds(h * (depth // 2), depth // 2)
            part = dn.at[slot, pl.ds(0, wide + narrow), lanes]
        return part, dn_recv_sem.at[h, slot], (mix_z, sc_z)[h]

    def to_z(kind, slot, up, down, both=False):
        ref, recv, sems = piece(kind, slot)
        group = {"mi": "mix", "sc": "mix", "gu": "gu", "dn": "dn"}[kind[:2]]
        if up is not None:
            start(remote(ref, ref, sems.at[slot], recv, to_up), up, group)
        if down is not None:
            at = shards + lax.rem(slot, 2) if both else slot
            start(remote(ref, ref, sems.at[at], recv, to_down), down, group)

    def wait_piece(kind, slot, cond=None):
        ref, recv, _ = piece(kind, slot)
        copy = remote(ref, ref, half_sem.at[0], recv, to_x)
        if cond is None:
            copy.wait_recv()
        else:
            pl.when(cond)(copy.wait_recv)

    def own_to_z(kind, slot):
        to_z(kind, slot, z < planes - 1, z > 0, both=True)

    def hop(kind, k, t, absolute=False, then=None):
        side = t if absolute else lax.rem(y + t, 2)
        for origin, has, up, down in (
            (z - k, z >= k, jnp.logical_and(z >= k, z < planes - 1), None),
            (z + k, z + k < planes, None, jnp.logical_and(z + k < planes, z > 0)),
        ):
            slot = jnp.clip(2 * origin + side, 0, shards - 1)
            wait_piece(kind, slot, has)
            if k < planes - 1:
                to_z(kind, slot, up, down)
            if then is not None:
                then(slot, has)

    def hop_gu(k, t):
        for kind in ("gu0", "gu1"):
            hop(kind, k, t)

    mine = mix_at(f, y_q)
    start(remote(mine, mine, mix_y.at[shards + y_q], mix_recv_at(f, y_q), to_y))
    own_to_z("mix", f)
    start(remote(scales.at[f], scales.at[f], y_sem.at[0], sc_recv_sem.at[f], to_y))
    own_to_z("sc", f)

    lane = lax.broadcasted_iota(jnp.int32, (depth, LANES), 1)

    def join(gate_tile, up_tile, side):
        shape = gate_tile.shape
        low_lane = lax.broadcasted_iota(jnp.int32, shape, 1) < narrow
        low = jnp.where(low_lane, gate_tile, pltpu.roll(up_tile, narrow, axis=1))
        high = jnp.where(low_lane, pltpu.roll(gate_tile, narrow, axis=1), up_tile)
        return jnp.where(side == 0, low, high)

    shift_of = wide + LANES

    def build_gu(side, write):
        write(0, wide, stage[0][:, lanes_at(side * shift_of, wide)].astype(bf16))
        write(wide, wide, stage[1][:, lanes_at(side * shift_of, wide)].astype(bf16))
        tile = join(stage[0][:, wide : wide + LANES], stage[1][:, wide : wide + LANES], side)
        write(2 * wide, LANES, tile.astype(bf16))

    def build_dn(side, write):
        for j in range(wide // LANES):
            tile = stage[2][:, lanes_at(side * shift_of + j * LANES, LANES)]
            write(j * LANES, LANES, tile.T.astype(bf16))
        tile = stage[2][:, wide : wide + LANES].T
        write(wide, narrow, jnp.where(side == 0, tile[:narrow], tile[narrow:]).astype(bf16))

    def write_gu_out(at, size, value):
        gu_out[:, at : at + size] = value

    def write_gu_own(at, size, value):
        gu[f, :, at : at + size] = value

    def write_dn_out(at, size, value):
        dn_out[at : at + size, :] = value

    def write_dn_own(at, size, value):
        dn[f, at : at + size, :] = value

    loads[2].wait()
    loads[3].wait()
    build_gu(y, write_gu_own)
    own_to_z("gu0", f)
    build_gu(1 - y, write_gu_out)
    for h in range(2):
        part = pl.ds(h * (depth // 2), depth // 2)
        there = gu.at[f, part, :]
        start(remote(gu_out.at[part, :], there, y_sem.at[1 + h], gu_recv_sem.at[h, f], to_y), None, "gu")
    wait_piece("mix", peer)
    own_to_z("mix", peer)
    wait_piece("sc", peer)
    own_to_z("sc", peer)

    def spread(slot, has):
        ref = mix_at(slot, own_q)
        start(remote(ref, ref, mix_x.at[slot], mix_recv_at(slot, own_q), to_x), has)
        start(remote(ref, ref, mix_y.at[slot], mix_recv_at(slot, own_q), to_y), has)

    for t in range(2):
        hop("mix", 1, t, then=spread)
        hop("sc", 1, t)

    loads[5].wait()
    small[2].wait()
    step_rows = 32

    @pl.loop(0, length // step_rows)
    def _(i):
        at = pl.ds(pl.multiple_of(i * step_rows, step_rows), step_rows)
        floats = tok[at, :].astype(f32)
        scaled = floats * lax.rsqrt(jnp.mean(floats * floats, axis=-1, keepdims=True) + epsilon)
        value = (scaled * gain1[...]).astype(bf16)
        for d in range(shards):
            normed[d, at, :] = value[:, d * depth : (d + 1) * depth]

    for k in range(2, planes):
        for t in range(2):
            hop("mix", k, t, then=spread)
            hop("sc", k, t)
        if k == planes - 2:
            own_to_z("gu1", f)
    for q in (own_q, x_q, far_q):
        ref = mix_at(f, q)
        start(remote(ref, ref, mix_y.at[shards + q], mix_recv_at(f, q), to_y))

    loads[4].wait()
    build_dn(1 - y, write_dn_out)
    build_dn(y, write_dn_own)

    @pl.loop(0, acc.shape[0] // 32)
    def _(r):
        acc[pl.ds(pl.multiple_of(r * 32, 32), 32), :] = jnp.zeros((32, span), f32)

    start(remote(dn_out, dn.at[f, pl.ds(0, wide + narrow), :], y_sem.at[3], half_sem.at[2], to_y), None, "gu")

    def wait_mix(slot, q, cond=None):
        ref = mix_at(slot, q)
        copy = remote(ref, ref, half_sem.at[0], mix_recv_at(slot, q), to_x)
        if cond is None:
            copy.wait_recv()
        else:
            pl.when(cond)(copy.wait_recv)

    def others(k, t, do):
        for origin, has in ((z - k, z >= k), (z + k, z + k < planes)):
            do(jnp.clip(2 * origin + lax.rem(y + t, 2), 0, shards - 1), has)

    def corner(slot, has):
        wait_mix(slot, y_q, has)
        ref = mix_at(slot, y_q)
        start(remote(ref, ref, mix_corner.at[slot], mix_recv_at(slot, y_q), to_x), has)

    def rest(slot, has):
        wait_mix(slot, x_q, has)
        wait_mix(slot, far_q, has)

    for kind in ("gu0", "gu1"):
        wait_piece(kind, peer)
        own_to_z(kind, peer)
    for k in range(1, planes):
        for t in range(2):
            others(k, 1 - t, corner)
    hop_gu(1, 0)
    for k in range(1, planes):
        for t in range(2):
            others(k, t, rest)
    for q in (y_q, x_q, far_q):
        wait_mix(peer, q)

    for load in small[3:]:
        load.wait()
    pool[...] = jnp.zeros(pool.shape, f32)

    @pl.loop(0, shards)
    def _(d):
        pool[...] += jnp.dot(normed[d], mix[0, d], preferred_element_type=f32)

    local_width = pool.shape[1]
    place = lax.broadcasted_iota(jnp.int32, (length, LANES), 0)
    for q in range(local_width // LANES):
        at = slice(q * LANES, (q + 1) * LANES)
        value = (pool[:, at] * in_scale[:, at]).astype(bf16).astype(f32)
        group = lax.div(c * local_width + q * LANES, POOL_GROUP)
        sums = value
        mean = jnp.zeros_like(value)
        for index in range(4):
            window = 2 ** (index + 1)
            shift = window // 2
            sums = sums + jnp.where(place >= shift, pltpu.roll(sums, shift, axis=0), 0.0)
            counts = jnp.minimum(place + 1, window).astype(f32)
            mean = jnp.where(group == index, sums / counts, mean)
        pooled = (mean - value).astype(bf16)
        mixed = jnp.dot(pooled, group_mix[:, at].astype(bf16), preferred_element_type=f32)
        grp[:, at] = (mixed * group_scale[:, at]).astype(bf16)

    def mixer_rows(d, core):
        left = grp[pl.ds(pl.multiple_of(core * rows, rows), rows), :]
        value = lax.dot_general(
            left, mix[1, d], (((1,), (1,)), ((), ())), preferred_element_type=f32
        )
        return (value * scales[d, 0:1, :]).astype(bf16)

    @pl.loop(0, shards)
    def _(d):
        mix_send[d] = mixer_rows(d, 1 - c)

    remote(mix_send, mix_recv, half_sem.at[0], half_sem.at[1], to_core).start()
    hop_gu(1, 1)

    @pl.loop(0, shards)
    def _(d):
        mid[d] = mixer_rows(d, c)

    remote(mix_send, mix_recv, half_sem.at[0], half_sem.at[1], to_core).wait_recv()
    my_rows = pl.ds(pl.multiple_of(c * rows, rows), rows)
    block = 2 * (2 * x + y) + c
    for part in range(4):
        size = rows // 4
        at = pl.ds(part * size, size)
        tok_at = pl.ds(pl.multiple_of(c * rows + part * size, size), size)
        squares = jnp.zeros((size, depth), f32)
        for d in range(shards):
            value = (
                tok[tok_at, d * depth : (d + 1) * depth].astype(f32)
                + (mid[d, at, :].astype(f32) + mix_recv[d, at, :].astype(f32))
            ).astype(bf16)
            mid[d, at, :] = value
            wide_value = value.astype(f32)
            squares = squares + wide_value * wide_value
        mean = jnp.sum(squares, axis=-1, keepdims=True) / (shards * depth)
        factor = lax.rsqrt(mean + epsilon)
        to_at = pl.ds(pl.multiple_of(block * rows + part * size, size), size)
        for d in range(shards):
            scaled = mid[d, at, :].astype(f32) * factor
            gain = gain2[:, d * depth : (d + 1) * depth]
            xb[d, to_at, :] = (scaled * gain).astype(bf16)

    half = rows // 2

    def rows_of(core, bx, by, h=None):
        first = (2 * (2 * bx + by) + core) * rows
        if h is None:
            return xb.at[:, pl.ds(pl.multiple_of(first, rows), rows), :]
        return xb.at[:, pl.ds(pl.multiple_of(first + h * half, half), half), :]

    def send_rows(ref, i, j, device):
        start(remote(ref, ref, tok_send.at[i], tok_recv.at[j], device), None, "tok")

    def wait_rows(ref, j):
        remote(ref, ref, half_sem.at[0], tok_recv.at[j], to_x).wait_recv()

    own_group = own_q
    settle("mix")

    orders = []
    for plane in range(planes):
        near = sorted(range(planes), key=lambda p: (abs(p - plane), p))
        orders.append(near)

    def plane_at(j):
        value = jnp.int32(0)
        for plane in range(planes):
            for i in range(planes):
                here = jnp.logical_and(z == plane, j == i)
                value = jnp.where(here, orders[plane][i], value)
        return value

    def unit(group, j):
        at = pl.ds(pl.multiple_of(group * 2 * rows, 2 * rows), 2 * rows)
        slot = 2 * plane_at(j)
        value = jnp.dot(xb[slot, at, :], gu[slot], preferred_element_type=f32)
        value += jnp.dot(xb[slot + 1, at, :], gu[slot + 1], preferred_element_type=f32)
        acc[at, :] += value

    for h in range(2):
        send_rows(rows_of(c, x, y, h), h, h, to_x)
        send_rows(rows_of(c, x, y, 1 - h), 2 + h, 2 + 1 - h, to_y)
    send_rows(rows_of(c, x, y), 4, 6, to_core)
    wait_rows(rows_of(1 - c, x, y), 6)

    @pl.loop(0, 2)
    def _(j):
        unit(own_group, j)

    hop_gu(2, 0)
    wait_rows(rows_of(c, 1 - x, y, 0), 0)
    send_rows(rows_of(c, 1 - x, y, 0), 5, 4, to_y)
    wait_rows(rows_of(c, x, 1 - y, 1), 3)
    send_rows(rows_of(c, x, 1 - y, 1), 6, 5, to_x)
    wait_rows(rows_of(c, 1 - x, y, 1), 1)
    send_rows(rows_of(c, 1 - x, y), 7, 7, to_core)
    wait_rows(rows_of(c, x, 1 - y, 0), 2)
    send_rows(rows_of(c, x, 1 - y), 8, 8, to_core)
    hop_gu(2, 1)
    remote(dn_out, dn.at[peer, pl.ds(0, wide + narrow), :], y_sem.at[3], half_sem.at[2], to_y).wait_recv()
    own_to_z("dn", 2 * z)
    own_to_z("dna", 2 * z + 1)
    own_to_z("dnb", 2 * z + 1)
    all_rows = xb.shape[1]
    tall = 512
    unit(own_group, 2)
    wait_rows(rows_of(1 - c, 1 - x, y), 7)
    wait_rows(rows_of(1 - c, x, 1 - y), 8)

    @pl.loop(0, 2)
    def _(g):
        group = jnp.where(g == 0, x_q, y_q)

        @pl.loop(0, planes - 1)
        def _(j):
            unit(group, j)

    wait_rows(rows_of(c, 1 - x, 1 - y, 0), 4)
    wait_rows(rows_of(c, 1 - x, 1 - y, 1), 5)
    send_rows(rows_of(c, 1 - x, 1 - y), 9, 9, to_core)
    wait_rows(rows_of(1 - c, 1 - x, 1 - y), 9)

    @pl.loop(0, planes - 1)
    def _(j):
        unit(far_q, j)

    for t in range(2):
        hop_gu(planes - 1, t)

        @pl.loop(0, 4)
        def _(g):
            at = pl.ds(pl.multiple_of(g * 2 * rows, 2 * rows), 2 * rows)
            slot = 2 * plane_at(planes - 1) + lax.rem(y + t, 2)
            acc[at, :] += jnp.dot(xb[slot, at, :], gu[slot], preferred_element_type=f32)

    wide_tiles = wide // LANES
    first_row = x * (span // LANES)
    joint_row = pl.ds(first_row + wide_tiles, 1)
    joint_scale = join(
        jnp.broadcast_to(gate_scale[joint_row, :], (8, LANES)),
        jnp.broadcast_to(up_scale[joint_row, :], (8, LANES)),
        y,
    )[0:1]
    gate_rows, up_rows = [], []
    for j in range(wide_tiles):
        at = pl.ds(first_row + y * (wide_tiles + 1) + j, 1)
        gate_rows.append(gate_scale[at, :])
        up_rows.append(up_scale[at, :])
    act = 64

    @pl.loop(0, all_rows // act)
    def _(r):
        at = pl.ds(pl.multiple_of(r * act, act), act)
        group = lax.div(r * act, 2 * rows)
        core = lax.rem(lax.div(r * act, rows), 2)
        inside = lax.rem(r * act, rows)
        to = pl.ds(pl.multiple_of(core * 4 * rows + group * rows + inside, act), act)
        for j in range(wide_tiles):
            cols = slice(j * LANES, (j + 1) * LANES)
            gate = acc[at, cols] * gate_rows[j]
            up = acc[at, wide + j * LANES : wide + (j + 1) * LANES] * up_rows[j]
            hid[to, cols] = (gate / (1.0 + jnp.exp(-gate)) * up).astype(bf16)
        both = acc[at, 2 * wide :] * joint_scale
        value = both / (1.0 + jnp.exp(-both)) * pltpu.roll(both, narrow, axis=1)
        keep = lax.broadcasted_iota(jnp.int32, (act, LANES), 1) < narrow
        hid[to, wide:] = jnp.where(keep, value, 0.0).astype(bf16)

    core_rows = all_rows // 2
    own = acc.at[pl.ds(0, core_rows), pl.ds(0, depth)]
    remote(mix_send, mix_recv, half_sem.at[0], half_sem.at[1], to_core).wait_send()
    cut = rows // 2
    chunks = [(i, 0, depth) for i in range(shards - 1)]
    chunks += [(shards - 1, 0, depth // 2), (shards - 1, depth // 2, depth // 2)]
    count = len(chunks)

    def views(i):
        p, at, size = chunks[i]
        return p, p % 2, slice(at, at + size), pl.ds(at, size)

    def slot_at(p):
        return 2 * plane_at(p // 2) + p % 2

    def sems(kind, i):
        p, at, _ = chunks[i]
        j = p % 2 if at == 0 else 2
        send = mix_y.at[3 * kind + j] if kind < 4 else mix_x.at[3 * (kind - 4) + j]
        return send, recv_sem.at[kind * count + i]

    def cs_copy(i):
        p, s, _, ln = views(i)
        source = normed.at[pl.ds(2 * s, 2), :, ln]
        return remote(source, cs_recv.at[p, :, :, ln], *sems(0, i), to_core)

    def bx_copy(i):
        p, s, _, ln = views(i)
        return remote(bx_send.at[s, :, :, ln], bx_recv.at[p, :, :, ln], *sems(1, i), to_x)

    def by_copy(i):
        p, s, _, ln = views(i)
        return remote(by_send.at[s, :, :, ln], by_recv.at[p, :, :, ln], *sems(2, i), to_y)

    def cx_copy(i):
        p, s, _, ln = views(i)
        return remote(cx_send.at[s, :, ln], cx_recv.at[p, :, ln], *sems(3, i), to_x)

    def cy_copy(i):
        p, s, _, ln = views(i)
        return remote(cy_send.at[s, :, ln], cy_recv.at[p, :, ln], *sems(4, i), to_y)

    def out_lanes(i):
        p, at, size = chunks[i]
        return lanes_at(slot_at(p) * depth + at, size)

    def out_copy(i, core=c):
        part = out.at[pl.ds(pl.multiple_of(core * rows, rows), rows), out_lanes(i)]
        return remote(part, part, *sems(5, i), to_core)

    def reused(i, make):
        p, at, _ = chunks[i]
        if p >= 2 and at == 0:
            make(p - 2).wait_send()

    def send_stage(i):
        p, s, cols, _ = views(i)
        slot = slot_at(p)
        reused(i, cs_copy)

        @pl.loop(0, core_rows // tall)
        def _(r):
            there = pl.ds(pl.multiple_of((1 - c) * core_rows + r * tall, tall), tall)
            value = jnp.dot(hid[there, :], dn[slot, :, cols], preferred_element_type=f32)
            normed[2 * s + r, :, cols] = value.astype(bf16)

        cs_copy(i).start()

    def own_stage(i):
        p, _, cols, _ = views(i)
        slot = slot_at(p)

        @pl.loop(0, core_rows // tall)
        def _(r):
            at = pl.ds(pl.multiple_of(r * tall, tall), tall)
            here = pl.ds(pl.multiple_of(c * core_rows + r * tall, tall), tall)
            own[at, cols] = jnp.dot(hid[here, :], dn[slot, :, cols], preferred_element_type=f32)

    def block_rows(bx, by, part):
        first = pl.multiple_of((2 * bx + by) * rows + part * cut, cut)
        inside = pl.multiple_of(by * rows + part * cut, cut)
        return pl.ds(first, cut), bx, pl.ds(inside, cut)

    def second_stage(i):
        p, s, cols, _ = views(i)
        cs_copy(i).wait_recv()
        reused(i, bx_copy)
        reused(i, by_copy)

        def total(block):
            at, pair, inside = block
            return own[at, cols] + cs_recv[p, pair, inside, cols].astype(f32)

        for b in range(2):
            bx_send[s, b, :, cols] = total(block_rows(1 - x, b, 0)).astype(bf16)
        bx_copy(i).start()
        for b in range(2):
            by_send[s, b, :, cols] = total(block_rows(b, 1 - y, 1)).astype(bf16)
        by_copy(i).start()
        for b in range(2):
            keep_l[s, b, :, cols] = total(block_rows(x, b, 0))
            keep_r[s, b, :, cols] = total(block_rows(b, y, 1))

    def third_stage(i):
        p, s, cols, _ = views(i)
        reused(i, cx_copy)
        reused(i, cy_copy)
        bx_copy(i).wait_recv()

        def left(b):
            return keep_l[s, b, :, cols] + bx_recv[p, b, :, cols].astype(f32)

        def right(b):
            return keep_r[s, b, :, cols] + by_recv[p, b, :, cols].astype(f32)

        cy_send[s, :, cols] = left(1 - y).astype(bf16)
        cy_copy(i).start()
        by_copy(i).wait_recv()
        cx_send[s, :, cols] = right(1 - x).astype(bf16)
        cx_copy(i).start()
        last_l[s, :, cols] = left(y)
        last_r[s, :, cols] = right(x)

    def fourth_stage(i):
        p, s, cols, _ = views(i)
        d = slot_at(p)
        scale = scales[d, 1:2, cols]
        for copy, last, recv, at in (
            (cy_copy(i), last_l, cy_recv, slice(0, cut)),
            (cx_copy(i), last_r, cx_recv, slice(cut, rows)),
        ):
            copy.wait_recv()
            total = last[s, :, cols] + recv[p, :, cols].astype(f32)
            value = (mid[d, at, cols].astype(f32) + total * scale).astype(bf16)
            first = pl.multiple_of(c * rows + at.start, cut)
            out[pl.ds(first, cut), out_lanes(i)] = value
        reused(i, out_copy)
        out_copy(i).start()

    stages = {0: send_stage, 1: own_stage, 2: second_stage, 3: third_stage, 4: fourth_stage}
    done = set()

    def run(stage, i):
        if i < 0 or i >= count or (stage, i) in done:
            return
        done.add((stage, i))
        stages[stage](i)

    for i in range(shards - 2):
        if i >= 2:
            for kind in ("dn",) if i % 2 == 0 else ("dna", "dnb"):
                hop(kind, i // 2, i % 2, absolute=True)
        run(0, i)
        run(1, i)
        run(4, i - 4)
        run(3, i - 2)
        run(2, i)
    n = shards - 2
    for stage, i in ((4, n - 4), (3, n - 2), (4, n - 3), (3, n - 1)):
        run(stage, i)
    settle("gu")
    settle("tok")
    hop("dn", planes - 1, 0, absolute=True)
    for stage, i in ((0, n), (1, n), (2, n), (4, n - 2), (4, n - 1)):
        run(stage, i)
    hop("dna", planes - 1, 1, absolute=True)
    for stage, i in ((0, n + 1), (1, n + 1), (2, n + 1)):
        run(stage, i)
    hop("dnb", planes - 1, 1, absolute=True)
    for stage, i in ((0, n + 2), (3, n), (1, n + 2), (2, n + 2), (3, n + 1), (4, n), (3, n + 2)):
        run(stage, i)
    run(4, n + 1)
    run(4, n + 2)

    settle("dn")
    for i in range(shards - 2, count):
        for make in (cs_copy, bx_copy, by_copy, cx_copy, cy_copy, out_copy):
            make(i).wait_send()
    for i in range(count):
        out_copy(i, 1 - c).wait_recv()


def make_fast(shards):
    planes = shards // 2

    def body(
        tokens,
        mixer_gain,
        pool_input,
        input_scale,
        group_mix,
        group_scale,
        pool_output,
        output_scale,
        channel_gain,
        gate_weight,
        gate_scale,
        up_weight,
        up_scale,
        down_weight,
        down_scale,
    ):
        f32, bf16 = jnp.float32, jnp.bfloat16
        length, width = tokens.shape
        depth, local_width = pool_input.shape
        span = gate_weight.shape[1] // 2
        padded = (span // 2 + LANES - 1) // LANES * LANES
        rows = length // 2
        everything = 8 * rows
        anywhere = pl.BlockSpec(memory_space=pl.ANY)
        dma = pltpu.SemaphoreType.DMA
        scratch = [
            pltpu.VMEM((1, width), f32),
            pltpu.VMEM((1, local_width), f32),
            pltpu.VMEM((1, local_width), f32),
            pltpu.VMEM((1, depth), f32),
            pltpu.VMEM((1, width), f32),
            pltpu.VMEM((2 * span // LANES, LANES), f32),
            pltpu.VMEM((2 * span // LANES, LANES), f32),
            pltpu.VMEM((1, depth), f32),
            pltpu.VMEM(group_mix.shape, f32),
            pltpu.VMEM((length, width), bf16),
            pltpu.VMEM((2, shards, depth, local_width), bf16),
            pltpu.VMEM((shards, 2, depth), f32),
            pltpu.VMEM((shards, length, depth), bf16),
            pltpu.VMEM((shards, depth, span), bf16),
            pltpu.VMEM((shards, padded, depth), bf16),
            pltpu.VMEM((depth, span), bf16),
            pltpu.VMEM((span // 2, depth), bf16),
            pltpu.VMEM((shards, everything, depth), bf16),
            pltpu.VMEM((everything, span), f32),
            pltpu.VMEM((everything, padded), bf16),
            pltpu.VMEM((length, local_width), f32),
            pltpu.VMEM((length, local_width), bf16),
            pltpu.VMEM((shards, rows, depth), bf16),
            pltpu.VMEM((shards, rows, depth), bf16),
            pltpu.VMEM((shards, rows, depth), bf16),
            pltpu.VMEM((shards, 2, 2 * rows, depth), bf16),
            pltpu.VMEM((2, 2, rows // 2, depth), bf16),
            pltpu.VMEM((shards, 2, rows // 2, depth), bf16),
            pltpu.VMEM((2, 2, rows // 2, depth), bf16),
            pltpu.VMEM((shards, 2, rows // 2, depth), bf16),
            pltpu.VMEM((2, rows // 2, depth), bf16),
            pltpu.VMEM((shards, rows // 2, depth), bf16),
            pltpu.VMEM((2, rows // 2, depth), bf16),
            pltpu.VMEM((shards, rows // 2, depth), bf16),
            pltpu.VMEM((2, 2, rows // 2, depth), f32),
            pltpu.VMEM((2, 2, rows // 2, depth), f32),
            pltpu.VMEM((2, rows // 2, depth), f32),
            pltpu.VMEM((2, rows // 2, depth), f32),
            dma((6 * (shards + 1),)),
            dma((shards + 2,)),
            dma((shards + 2,)),
            dma((2, shards + 2)),
            dma((shards,)),
            dma((2, shards)),
            dma((2, shards)),
            dma((shards,)),
            dma((shards,)),
            dma((shards + 4,)),
            dma((4,)),
            dma((3,)),
            dma((10,)),
            dma((10,)),
        ]
        row = lambda value: value.reshape(1, -1)
        return pl.pallas_call(
            functools.partial(layer_kernel, planes),
            name="layer",
            out_shape=pltpu.VMEM((length, width), bf16),
            in_specs=[anywhere] * 15,
            out_specs=pl.BlockSpec(memory_space=pltpu.VMEM),
            scratch_shapes=scratch,
            compiler_params=pltpu.CompilerParams(
                collective_id=0, has_side_effects=True, vmem_limit_bytes=60 * 2**20
            ),
        )(
            tokens,
            row(mixer_gain),
            row(input_scale),
            row(group_scale),
            row(output_scale),
            row(channel_gain),
            gate_scale.reshape(-1, LANES),
            up_scale.reshape(-1, LANES),
            row(down_scale),
            group_mix,
            pool_input,
            pool_output,
            gate_weight,
            up_weight,
            down_weight,
        )

    return body


def solution(mesh):
    in_specs = (
        P(("rep", "fs"), None),
        P(),
        P("fs", "tp"),
        P("tp"),
        P(None, "tp"),
        P("tp"),
        P("fs", "tp"),
        P("fs"),
        P(),
        P("fs", "tp"),
        P("tp"),
        P("fs", "tp"),
        P("tp"),
        P("fs", "tp"),
        P("fs"),
    )
    out_specs = P(("rep", "fs"), None)
    reps, shards, cores = mesh.shape["rep"], mesh.shape["fs"], mesh.shape["tp"]
    fast = reps == 2 and cores == 2 and shards % 2 == 0 and shards >= 8
    body = make_fast(shards) if fast else make_body(reps, shards, cores)
    return jax.shard_map(body, mesh=mesh, in_specs=in_specs, out_specs=out_specs, check_vma=False)
```

```python
import functools

import jax
import jax.numpy as jnp
from jax import lax
from jax.experimental import pallas as pl
from jax.experimental.pallas import tpu as pltpu
from jax.sharding import PartitionSpec as P

POOL_GROUP = 256

epsilon = 1e-06


def normed_rows(floats, gain_row):
    scaled = floats * lax.rsqrt(jnp.mean(floats * floats, axis=-1, keepdims=True) + epsilon)
    return (scaled * gain_row).astype(jnp.bfloat16)


def product(left_rows, weight):
    return jnp.dot(left_rows, weight, preferred_element_type=jnp.float32)


def transposed_product(left_rows, weight_rows):
    return lax.dot_general(
        left_rows, weight_rows, (((1,), (1,)), ((), ())), preferred_element_type=jnp.float32
    )


def thirds(scale):
    high = lax.reduce_precision(scale, 8, 7)
    rest = scale - high
    middle = lax.reduce_precision(rest, 8, 7)
    return [piece.astype(jnp.bfloat16) for piece in (high, middle, rest - middle)]


def make_body(reps, shards, cores):
    def over_rep(value):
        return lax.ppermute(value, "rep", [(i, (i + 1) % reps) for i in range(reps)])

    def over_pair(value):
        return lax.ppermute(value, "fs", [(i, i ^ 1) for i in range(shards)])

    def over_cores(value):
        return lax.ppermute(value, "tp", [(0, 1), (1, 0)])

    def sum_cores(value):
        if cores == 2:
            core = lax.axis_index("tp")
            rows = value.shape[0] // 2
            other = lax.dynamic_slice_in_dim(value, (1 - core) * rows, rows, 0)
            own = lax.dynamic_slice_in_dim(value, core * rows, rows, 0)
            other = lax.ppermute(other.astype(jnp.bfloat16), "tp", [(0, 1), (1, 0)])
            own = lax.optimization_barrier(own.astype(jnp.bfloat16))
            return own.astype(jnp.float32) + other.astype(jnp.float32)
        total = lax.psum_scatter(
            value.astype(jnp.bfloat16), "tp", scatter_dimension=0, tiled=True
        )
        return total.astype(jnp.float32)

    def gather_cores(value):
        if cores == 2:
            core = lax.axis_index("tp")
            other = lax.ppermute(value, "tp", [(0, 1), (1, 0)])
            first = jnp.where(core == 0, value, other)
            second = jnp.where(core == 0, other, value)
            return jnp.concatenate([first, second], axis=0)
        return lax.all_gather(value, "tp", axis=0, tiled=True)

    lines = [[i for i in range(shards) if i % 2 == side] for side in range(2)]

    def body(
        tokens,
        mixer_gain,
        pool_input,
        input_scale,
        group_mix,
        group_scale,
        pool_output,
        output_scale,
        channel_gain,
        gate_weight,
        gate_scale,
        up_weight,
        up_scale,
        down_weight,
        down_scale,
    ):
        rep = lax.axis_index("rep")
        side = lax.axis_index("fs") % 2
        core = lax.axis_index("tp")
        length = tokens.shape[0]
        block_width = group_mix.shape[0]
        local_width = group_mix.shape[1]

        def arranged(own, peer):
            low = jnp.where(side == 0, own, peer)
            high = jnp.where(side == 0, peer, own)
            return low, high

        def share_of(weight, which):
            share = weight.shape[-1] // (2 * reps)
            return lax.dynamic_slice_in_dim(
                weight, (rep * 2 + which) * share, share, weight.ndim - 1
            )

        def shares(weights, which):
            return [share_of(weight, which).astype(jnp.bfloat16) for weight in weights]

        def along_line(block):
            return lax.all_gather(block, "fs", axis=0, tiled=True, axis_index_groups=lines)

        columns = jnp.stack(thirds(output_scale) + thirds(down_scale), axis=1)
        columns = jnp.pad(columns, ((0, 0), (0, 128 - columns.shape[1])))
        mixer_weights = (pool_input, pool_output)
        keep = jnp.concatenate(shares(mixer_weights, side) + [columns], axis=1)
        send = jnp.concatenate(shares(mixer_weights, 1 - side) + [columns], axis=1)
        mine = along_line(jnp.concatenate(arranged(keep, over_pair(send)), axis=0))

        channel_weights = (gate_weight, up_weight, down_weight)
        keep = jnp.concatenate(shares(channel_weights, side), axis=1)
        send = jnp.concatenate(shares(channel_weights, 1 - side), axis=1)
        low, high = arranged(keep, over_pair(send))
        width = keep.shape[1] // 3
        block = jnp.concatenate([low[:, : 2 * width], high[:, : 2 * width]], axis=0)
        block, low, high, mine = lax.optimization_barrier(
            (block, low[:, 2 * width :], high[:, 2 * width :], mine)
        )
        gate_up = along_line(block)
        down_parts = [along_line(low), along_line(high)]

        quarter = local_width // 4
        feature = mine[:, 2 * quarter : 2 * quarter + 6].astype(jnp.float32).T
        output_feature = feature[0:1] + feature[1:2] + feature[2:3]
        down_feature = feature[3:4] + feature[4:5] + feature[5:6]
        mine = mine[:, : 2 * quarter]
        by_rep = over_rep(mine)
        by_side = over_pair(mine)
        split = mine.shape[0] // 2
        by_both = jnp.concatenate([over_pair(by_rep[:split]), over_rep(by_side[split:])], axis=0)
        own_low, own_high = arranged(mine, by_side)
        peer_low, peer_high = arranged(by_rep, by_both)
        quarters = [
            jnp.where(rep == 0, own_low, peer_low),
            jnp.where(rep == 0, own_high, peer_high),
            jnp.where(rep == 0, peer_low, own_low),
            jnp.where(rep == 0, peer_high, own_high),
        ]
        input_full = jnp.concatenate([piece[:, :quarter] for piece in quarters], axis=1)
        output_full = jnp.concatenate([piece[:, quarter:] for piece in quarters], axis=1)

        normed = normed_rows(tokens.astype(jnp.float32), mixer_gain)
        pool_in = (product(normed, input_full) * input_scale).astype(jnp.bfloat16)
        places = jnp.arange(length, dtype=jnp.int32)
        window_sums = pool_in.astype(jnp.float32)
        channel_group = (
            core * local_width + jnp.arange(local_width, dtype=jnp.int32)
        ) // POOL_GROUP
        pooled_mean = jnp.zeros((length, local_width), jnp.float32)
        for group_index in range(4):
            window = 2 ** (group_index + 1)
            shift = window // 2
            window_sums = window_sums + jnp.pad(window_sums[:-shift], ((shift, 0), (0, 0)))
            counts = jnp.minimum(places + 1, window).astype(jnp.float32)
            pooled_mean = jnp.where(
                channel_group[None, :] == group_index, window_sums / counts[:, None], pooled_mean
            )
        pooled = (pooled_mean - pool_in.astype(jnp.float32)).astype(jnp.bfloat16)
        local_blocks = local_width // block_width
        mixed_raw = jnp.einsum(
            "sgc,cgd->sgd",
            pooled.reshape(length, local_blocks, block_width),
            group_mix.astype(jnp.bfloat16).reshape(block_width, local_blocks, block_width),
            preferred_element_type=jnp.float32,
        ).reshape(length, local_width)
        grouped = (mixed_raw * group_scale).astype(jnp.bfloat16)
        mixer_out = sum_cores(transposed_product(grouped, output_full) * output_feature)

        rows = length // cores
        own_tokens = lax.dynamic_slice_in_dim(tokens, core * rows, rows, 0)
        middle = (own_tokens.astype(jnp.float32) + mixer_out).astype(jnp.bfloat16)
        middle = lax.optimization_barrier(middle)
        second = normed_rows(middle.astype(jnp.float32), channel_gain)

        from_rep = over_rep(second)
        from_side = over_pair(second)
        half_rows = rows // 2
        corner = jnp.concatenate(
            [over_pair(from_rep[:half_rows]), over_rep(from_side[half_rows:])], axis=0
        )
        member_rows = jnp.concatenate([second, from_rep, from_side, corner], axis=0)
        if cores == 2:
            row_sets = [over_cores(member_rows), member_rows]
        else:
            row_sets = [lax.all_gather(member_rows, "tp", axis=0, tiled=True)]

        def activated(row_set):
            both = product(row_set, gate_up)
            gate_sum = both[:, :width] * share_of(gate_scale, side)
            up_sum = both[:, width:] * share_of(up_scale, side)
            return (jax.nn.silu(gate_sum) * up_sum).astype(jnp.bfloat16)

        hidden_sets = lax.optimization_barrier([activated(row_set) for row_set in row_sets])

        def wide(value):
            return value.astype(jnp.float32)

        def scattered(down_part, hidden_sets):
            partials = [
                transposed_product(hidden, down_part).astype(jnp.bfloat16)
                for hidden in hidden_sets
            ]
            if cores == 2:
                summed = wide(over_cores(partials[0])) + wide(partials[1])
            else:
                summed = wide(
                    lax.psum_scatter(partials[0], "tp", scatter_dimension=0, tiled=True)
                )
            partial = summed.astype(jnp.bfloat16).reshape(4, rows, -1)
            half = partial.shape[2] // 2
            left, right = partial[:, :, :half], partial[:, :, half:]
            left_two = wide(left[0::2]) + wide(over_rep(left[1::2]))
            right_two = wide(right[:2]) + wide(over_pair(right[2:]))
            left_last = wide(over_pair(left_two[1].astype(jnp.bfloat16)))
            right_last = wide(over_rep(right_two[1].astype(jnp.bfloat16)))
            total = jnp.concatenate([left_two[0] + left_last, right_two[0] + right_last], axis=1)
            return total.reshape(rows, shards // 2, -1)

        low_total = scattered(down_parts[0], hidden_sets)
        low_total, hidden_sets = lax.optimization_barrier((low_total, hidden_sets))
        high_total = scattered(down_parts[1], hidden_sets)
        total = jnp.stack([low_total, high_total], axis=2)
        total = total.reshape(rows, -1)
        own_out = (middle.astype(jnp.float32) + total * down_feature).astype(jnp.bfloat16)
        return gather_cores(own_out)

    return body


MESH = pl.DeviceIdType.MESH
LANES = 128


def remote(src, dst, send, recv, device):
    return pltpu.make_async_remote_copy(
        src_ref=src,
        dst_ref=dst,
        send_sem=send,
        recv_sem=recv,
        device_id=device,
        device_id_type=MESH,
    )


def lanes_at(start, width):
    return pl.ds(pl.multiple_of(start, LANES), width)


def layer_kernel(
    planes,
    tok_any,
    gain1_any,
    in_scale_any,
    group_scale_any,
    out_scale_any,
    gain2_any,
    gate_scale_any,
    up_scale_any,
    down_scale_any,
    group_mix_any,
    pool_in_any,
    pool_out_any,
    gate_any,
    up_any,
    down_any,
    out,
    gain1,
    in_scale,
    group_scale,
    out_scale,
    gain2,
    gate_scale,
    up_scale,
    down_scale,
    group_mix,
    tok,
    mix,
    scales,
    normed,
    gu,
    dn,
    gu_out,
    dn_out,
    xb,
    acc,
    hid,
    pool,
    grp,
    mix_send,
    mix_recv,
    mid,
    cs_recv,
    bx_send,
    bx_recv,
    by_send,
    by_recv,
    cx_send,
    cx_recv,
    cy_send,
    cy_recv,
    keep_l,
    keep_r,
    last_l,
    last_r,
    recv_sem,
    mix_z,
    sc_z,
    gu_z,
    sc_recv_sem,
    gu_recv_sem,
    dn_recv_sem,
    mix_x,
    mix_corner,
    mix_y,
    y_sem,
    half_sem,
    tok_recv,
):
    f32, bf16 = jnp.float32, jnp.bfloat16
    x = lax.axis_index("rep")
    f = lax.axis_index("fs")
    c = lax.axis_index("tp")
    y = lax.rem(f, 2)
    z = lax.div(f, 2)
    shards = 2 * planes
    depth = mix.shape[2]
    quarter = mix.shape[3] // 4
    rows = mid.shape[1]
    length = tok.shape[0]
    span = gu.shape[2]
    wide = span // 2 // LANES * LANES
    narrow = span // 2 - wide
    to_x = (1 - x, f, c)
    to_y = (x, 2 * z + 1 - y, c)
    to_up = (x, f + 2, c)
    to_down = (x, f - 2, c)
    to_core = (x, f, 1 - c)
    peer = 2 * z + 1 - y
    own_q = 2 * x + y
    y_q = 2 * x + 1 - y
    x_q = 2 * (1 - x) + y
    far_q = 2 * (1 - x) + 1 - y
    sends = []

    def start(copy, cond=None, group="mix"):
        if cond is None:
            copy.start()
        else:
            pl.when(cond)(copy.start)
        sends.append((copy, cond, group))

    def settle(which):
        for copy, cond, group in sends:
            if group == which and cond is None:
                copy.wait_send()
            elif group == which:
                pl.when(cond)(copy.wait_send)

    stage = {}
    for i, ref in enumerate((gate_any, up_any, down_any)):
        stage[i] = acc.at[pl.ds(i * depth, depth), :]
    loads = [
        pltpu.make_async_copy(pool_in_any, pool.at[pl.ds(0, depth), :], recv_sem.at[4 * shards]),
        pltpu.make_async_copy(pool_out_any, pool.at[pl.ds(depth, depth), :], recv_sem.at[4 * shards + 1]),
    ]
    for i, ref in enumerate((gate_any, up_any, down_any)):
        loads.append(
            pltpu.make_async_copy(
                ref.at[:, lanes_at(x * span, span)], stage[i], recv_sem.at[4 * shards + 2 + i]
            )
        )
    loads.append(pltpu.make_async_copy(tok_any, tok, recv_sem.at[4 * shards + 5]))
    small = []
    for i, (source, target) in enumerate(
        (
            (out_scale_any, out_scale),
            (down_scale_any, down_scale),
            (gain1_any, gain1),
            (in_scale_any, in_scale),
            (group_scale_any, group_scale),
            (group_mix_any, group_mix),
            (gain2_any, gain2),
            (gate_scale_any, gate_scale),
            (up_scale_any, up_scale),
        )
    ):
        small.append(pltpu.make_async_copy(source, target, recv_sem.at[4 * shards + 6 + i]))
    for load in loads[:2] + small[:2] + loads[2:4] + small[2:] + loads[4:]:
        load.start()

    barrier = pltpu.get_barrier_semaphore()
    for device in (to_x, to_y, to_core):
        pl.semaphore_signal(barrier, inc=1, device_id=device, device_id_type=MESH)

    @pl.when(z > 0)
    def _():
        pl.semaphore_signal(barrier, inc=1, device_id=to_down, device_id_type=MESH)

    @pl.when(z < planes - 1)
    def _():
        pl.semaphore_signal(barrier, inc=1, device_id=to_up, device_id_type=MESH)

    loads[0].wait()
    mix[0, f] = pool[0:depth, :].astype(bf16)
    loads[1].wait()
    mix[1, f] = pool[depth : 2 * depth, :].astype(bf16)
    small[0].wait()
    scales[f, 0:1, :] = out_scale[...]
    small[1].wait()
    scales[f, 1:2, :] = down_scale[...]
    for d in range(shards):
        dn[d, wide + narrow :, :] = jnp.zeros((dn.shape[1] - wide - narrow, dn.shape[2]), bf16)
    pl.semaphore_wait(
        barrier, 3 + jnp.where(z > 0, 1, 0) + jnp.where(z < planes - 1, 1, 0)
    )

    def mix_recv_at(slot, q):
        return recv_sem.at[4 * slot + q]

    def mix_at(slot, q):
        return mix.at[:, slot, :, lanes_at(q * quarter, quarter)]

    def piece(kind, slot):
        if kind == "mix":
            return mix_at(slot, own_q), mix_recv_at(slot, own_q), mix_z
        if kind == "sc":
            return scales.at[slot], sc_recv_sem.at[slot], sc_z
        if kind in ("gu0", "gu1"):
            h = int(kind[2])
            part = gu.at[slot, pl.ds(h * (depth // 2), depth // 2), :]
            return part, gu_recv_sem.at[h, slot], gu_z.at[h]
        if kind == "dn":
            part, h = dn.at[slot, pl.ds(0, wide + narrow), :], 0
        else:
            h = ("dna", "dnb").index(kind)
            lanes = pl.ds(h * (depth // 2), depth // 2)
            part = dn.at[slot, pl.ds(0, wide + narrow), lanes]
        return part, dn_recv_sem.at[h, slot], (mix_z, sc_z)[h]

    def to_z(kind, slot, up, down, both=False):
        ref, recv, sems = piece(kind, slot)
        group = {"mi": "mix", "sc": "mix", "gu": "gu", "dn": "dn"}[kind[:2]]
        if up is not None:
            start(remote(ref, ref, sems.at[slot], recv, to_up), up, group)
        if down is not None:
            at = shards + lax.rem(slot, 2) if both else slot
            start(remote(ref, ref, sems.at[at], recv, to_down), down, group)

    def wait_piece(kind, slot, cond=None):
        ref, recv, _ = piece(kind, slot)
        copy = remote(ref, ref, half_sem.at[0], recv, to_x)
        if cond is None:
            copy.wait_recv()
        else:
            pl.when(cond)(copy.wait_recv)

    def own_to_z(kind, slot):
        to_z(kind, slot, z < planes - 1, z > 0, both=True)

    def hop(kind, k, t, absolute=False, then=None):
        side = t if absolute else lax.rem(y + t, 2)
        for origin, has, up, down in (
            (z - k, z >= k, jnp.logical_and(z >= k, z < planes - 1), None),
            (z + k, z + k < planes, None, jnp.logical_and(z + k < planes, z > 0)),
        ):
            slot = jnp.clip(2 * origin + side, 0, shards - 1)
            wait_piece(kind, slot, has)
            if k < planes - 1:
                to_z(kind, slot, up, down)
            if then is not None:
                then(slot, has)

    def hop_gu(k, t):
        for kind in ("gu0", "gu1"):
            hop(kind, k, t)

    mine = mix_at(f, y_q)
    start(remote(mine, mine, mix_y.at[shards + y_q], mix_recv_at(f, y_q), to_y))
    own_to_z("mix", f)
    start(remote(scales.at[f], scales.at[f], y_sem.at[0], sc_recv_sem.at[f], to_y))
    own_to_z("sc", f)

    lane = lax.broadcasted_iota(jnp.int32, (depth, LANES), 1)

    def join(gate_tile, up_tile, side):
        shape = gate_tile.shape
        low_lane = lax.broadcasted_iota(jnp.int32, shape, 1) < narrow
        low = jnp.where(low_lane, gate_tile, pltpu.roll(up_tile, narrow, axis=1))
        high = jnp.where(low_lane, pltpu.roll(gate_tile, narrow, axis=1), up_tile)
        return jnp.where(side == 0, low, high)

    shift_of = wide + LANES

    def build_gu(side, write):
        write(0, wide, stage[0][:, lanes_at(side * shift_of, wide)].astype(bf16))
        write(wide, wide, stage[1][:, lanes_at(side * shift_of, wide)].astype(bf16))
        tile = join(stage[0][:, wide : wide + LANES], stage[1][:, wide : wide + LANES], side)
        write(2 * wide, LANES, tile.astype(bf16))

    def build_dn(side, write):
        for j in range(wide // LANES):
            tile = stage[2][:, lanes_at(side * shift_of + j * LANES, LANES)]
            write(j * LANES, LANES, tile.T.astype(bf16))
        tile = stage[2][:, wide : wide + LANES].T
        write(wide, narrow, jnp.where(side == 0, tile[:narrow], tile[narrow:]).astype(bf16))

    def write_gu_out(at, size, value):
        gu_out[:, at : at + size] = value

    def write_gu_own(at, size, value):
        gu[f, :, at : at + size] = value

    def write_dn_out(at, size, value):
        dn_out[at : at + size, :] = value

    def write_dn_own(at, size, value):
        dn[f, at : at + size, :] = value

    loads[2].wait()
    loads[3].wait()
    build_gu(y, write_gu_own)
    own_to_z("gu0", f)
    build_gu(1 - y, write_gu_out)
    for h in range(2):
        part = pl.ds(h * (depth // 2), depth // 2)
        there = gu.at[f, part, :]
        start(remote(gu_out.at[part, :], there, y_sem.at[1 + h], gu_recv_sem.at[h, f], to_y), None, "gu")
    wait_piece("mix", peer)
    own_to_z("mix", peer)
    wait_piece("sc", peer)
    own_to_z("sc", peer)

    def spread(slot, has):
        ref = mix_at(slot, own_q)
        start(remote(ref, ref, mix_x.at[slot], mix_recv_at(slot, own_q), to_x), has)
        start(remote(ref, ref, mix_y.at[slot], mix_recv_at(slot, own_q), to_y), has)

    for t in range(2):
        hop("mix", 1, t, then=spread)
        hop("sc", 1, t)

    loads[5].wait()
    small[2].wait()
    step_rows = 32

    @pl.loop(0, length // step_rows)
    def _(i):
        at = pl.ds(pl.multiple_of(i * step_rows, step_rows), step_rows)
        floats = tok[at, :].astype(f32)
        scaled = floats * lax.rsqrt(jnp.mean(floats * floats, axis=-1, keepdims=True) + epsilon)
        value = (scaled * gain1[...]).astype(bf16)
        for d in range(shards):
            normed[d, at, :] = value[:, d * depth : (d + 1) * depth]

    for k in range(2, planes):
        for t in range(2):
            hop("mix", k, t, then=spread)
            hop("sc", k, t)
        if k == planes - 2:
            own_to_z("gu1", f)
    for q in (own_q, x_q, far_q):
        ref = mix_at(f, q)
        start(remote(ref, ref, mix_y.at[shards + q], mix_recv_at(f, q), to_y))

    loads[4].wait()
    build_dn(1 - y, write_dn_out)
    build_dn(y, write_dn_own)

    @pl.loop(0, acc.shape[0] // 32)
    def _(r):
        acc[pl.ds(pl.multiple_of(r * 32, 32), 32), :] = jnp.zeros((32, span), f32)

    start(remote(dn_out, dn.at[f, pl.ds(0, wide + narrow), :], y_sem.at[3], half_sem.at[2], to_y), None, "gu")

    def wait_mix(slot, q, cond=None):
        ref = mix_at(slot, q)
        copy = remote(ref, ref, half_sem.at[0], mix_recv_at(slot, q), to_x)
        if cond is None:
            copy.wait_recv()
        else:
            pl.when(cond)(copy.wait_recv)

    def others(k, t, do):
        for origin, has in ((z - k, z >= k), (z + k, z + k < planes)):
            do(jnp.clip(2 * origin + lax.rem(y + t, 2), 0, shards - 1), has)

    def corner(slot, has):
        wait_mix(slot, y_q, has)
        ref = mix_at(slot, y_q)
        start(remote(ref, ref, mix_corner.at[slot], mix_recv_at(slot, y_q), to_x), has)

    def rest(slot, has):
        wait_mix(slot, x_q, has)
        wait_mix(slot, far_q, has)

    for kind in ("gu0", "gu1"):
        wait_piece(kind, peer)
        own_to_z(kind, peer)
    for k in range(1, planes):
        for t in range(2):
            others(k, 1 - t, corner)
    hop_gu(1, 0)
    for k in range(1, planes):
        for t in range(2):
            others(k, t, rest)
    for q in (y_q, x_q, far_q):
        wait_mix(peer, q)

    for load in small[3:]:
        load.wait()
    pool[...] = jnp.zeros(pool.shape, f32)

    @pl.loop(0, shards)
    def _(d):
        pool[...] += jnp.dot(normed[d], mix[0, d], preferred_element_type=f32)

    local_width = pool.shape[1]
    place = lax.broadcasted_iota(jnp.int32, (length, LANES), 0)
    for q in range(local_width // LANES):
        at = slice(q * LANES, (q + 1) * LANES)
        value = (pool[:, at] * in_scale[:, at]).astype(bf16).astype(f32)
        group = lax.div(c * local_width + q * LANES, POOL_GROUP)
        sums = value
        mean = jnp.zeros_like(value)
        for index in range(4):
            window = 2 ** (index + 1)
            shift = window // 2
            sums = sums + jnp.where(place >= shift, pltpu.roll(sums, shift, axis=0), 0.0)
            counts = jnp.minimum(place + 1, window).astype(f32)
            mean = jnp.where(group == index, sums / counts, mean)
        pooled = (mean - value).astype(bf16)
        mixed = jnp.dot(pooled, group_mix[:, at].astype(bf16), preferred_element_type=f32)
        grp[:, at] = (mixed * group_scale[:, at]).astype(bf16)

    def mixer_rows(d, core):
        left = grp[pl.ds(pl.multiple_of(core * rows, rows), rows), :]
        value = lax.dot_general(
            left, mix[1, d], (((1,), (1,)), ((), ())), preferred_element_type=f32
        )
        return (value * scales[d, 0:1, :]).astype(bf16)

    @pl.loop(0, shards)
    def _(d):
        mix_send[d] = mixer_rows(d, 1 - c)

    remote(mix_send, mix_recv, half_sem.at[0], half_sem.at[1], to_core).start()
    hop_gu(1, 1)

    @pl.loop(0, shards)
    def _(d):
        mid[d] = mixer_rows(d, c)

    remote(mix_send, mix_recv, half_sem.at[0], half_sem.at[1], to_core).wait_recv()
    my_rows = pl.ds(pl.multiple_of(c * rows, rows), rows)
    block = 2 * (2 * x + y) + c
    for part in range(4):
        size = rows // 4
        at = pl.ds(part * size, size)
        tok_at = pl.ds(pl.multiple_of(c * rows + part * size, size), size)
        squares = jnp.zeros((size, depth), f32)
        for d in range(shards):
            value = (
                tok[tok_at, d * depth : (d + 1) * depth].astype(f32)
                + (mid[d, at, :].astype(f32) + mix_recv[d, at, :].astype(f32))
            ).astype(bf16)
            mid[d, at, :] = value
            wide_value = value.astype(f32)
            squares = squares + wide_value * wide_value
        mean = jnp.sum(squares, axis=-1, keepdims=True) / (shards * depth)
        factor = lax.rsqrt(mean + epsilon)
        to_at = pl.ds(pl.multiple_of(block * rows + part * size, size), size)
        for d in range(shards):
            scaled = mid[d, at, :].astype(f32) * factor
            gain = gain2[:, d * depth : (d + 1) * depth]
            xb[d, to_at, :] = (scaled * gain).astype(bf16)

    half = rows // 2

    def rows_of(core, bx, by, h=None):
        first = (2 * (2 * bx + by) + core) * rows
        if h is None:
            return xb.at[:, pl.ds(pl.multiple_of(first, rows), rows), :]
        return xb.at[:, pl.ds(pl.multiple_of(first + h * half, half), half), :]

    def send_rows(ref, i, j, device):
        sem = mix_corner.at[i] if i < 8 else mix_x.at[i - 2]
        start(remote(ref, ref, sem, tok_recv.at[j], device), None, "tok")

    def wait_rows(ref, j):
        remote(ref, ref, half_sem.at[0], tok_recv.at[j], to_x).wait_recv()

    own_group = own_q
    settle("mix")

    orders = []
    for plane in range(planes):
        near = sorted(range(planes), key=lambda p: (abs(p - plane), p))
        orders.append(near)

    def plane_at(j):
        value = jnp.int32(0)
        for plane in range(planes):
            for i in range(planes):
                here = jnp.logical_and(z == plane, j == i)
                value = jnp.where(here, orders[plane][i], value)
        return value

    def unit(group, j):
        at = pl.ds(pl.multiple_of(group * 2 * rows, 2 * rows), 2 * rows)
        slot = 2 * plane_at(j)
        value = jnp.dot(xb[slot, at, :], gu[slot], preferred_element_type=f32)
        value += jnp.dot(xb[slot + 1, at, :], gu[slot + 1], preferred_element_type=f32)
        acc[at, :] += value

    for h in range(2):
        send_rows(rows_of(c, x, y, h), h, h, to_x)
        send_rows(rows_of(c, x, y, 1 - h), 2 + h, 2 + 1 - h, to_y)
    send_rows(rows_of(c, x, y), 4, 6, to_core)
    wait_rows(rows_of(1 - c, x, y), 6)

    @pl.loop(0, 2)
    def _(j):
        unit(own_group, j)

    hop_gu(2, 0)
    wait_rows(rows_of(c, 1 - x, y, 0), 0)
    send_rows(rows_of(c, 1 - x, y, 0), 5, 4, to_y)
    wait_rows(rows_of(c, x, 1 - y, 1), 3)
    send_rows(rows_of(c, x, 1 - y, 1), 6, 5, to_x)
    wait_rows(rows_of(c, 1 - x, y, 1), 1)
    send_rows(rows_of(c, 1 - x, y), 7, 7, to_core)
    wait_rows(rows_of(c, x, 1 - y, 0), 2)
    send_rows(rows_of(c, x, 1 - y), 8, 8, to_core)
    hop_gu(2, 1)
    remote(dn_out, dn.at[peer, pl.ds(0, wide + narrow), :], y_sem.at[3], half_sem.at[2], to_y).wait_recv()
    own_to_z("dn", 2 * z)
    own_to_z("dna", 2 * z + 1)
    own_to_z("dnb", 2 * z + 1)
    all_rows = xb.shape[1]
    tall = 512
    unit(own_group, 2)
    wait_rows(rows_of(1 - c, 1 - x, y), 7)
    wait_rows(rows_of(1 - c, x, 1 - y), 8)

    @pl.loop(0, 2)
    def _(g):
        group = jnp.where(g == 0, x_q, y_q)

        @pl.loop(0, planes - 1)
        def _(j):
            unit(group, j)

    wait_rows(rows_of(c, 1 - x, 1 - y, 0), 4)
    wait_rows(rows_of(c, 1 - x, 1 - y, 1), 5)
    send_rows(rows_of(c, 1 - x, 1 - y), 9, 9, to_core)
    wait_rows(rows_of(1 - c, 1 - x, 1 - y), 9)

    @pl.loop(0, planes - 1)
    def _(j):
        unit(far_q, j)

    for t in range(2):
        hop_gu(planes - 1, t)

        @pl.loop(0, 4)
        def _(g):
            at = pl.ds(pl.multiple_of(g * 2 * rows, 2 * rows), 2 * rows)
            slot = 2 * plane_at(planes - 1) + lax.rem(y + t, 2)
            acc[at, :] += jnp.dot(xb[slot, at, :], gu[slot], preferred_element_type=f32)

    wide_tiles = wide // LANES
    first_row = x * (span // LANES)
    joint_row = pl.ds(first_row + wide_tiles, 1)
    joint_scale = join(
        jnp.broadcast_to(gate_scale[joint_row, :], (8, LANES)),
        jnp.broadcast_to(up_scale[joint_row, :], (8, LANES)),
        y,
    )[0:1]
    gate_rows, up_rows = [], []
    for j in range(wide_tiles):
        at = pl.ds(first_row + y * (wide_tiles + 1) + j, 1)
        gate_rows.append(gate_scale[at, :])
        up_rows.append(up_scale[at, :])
    act = 64

    @pl.loop(0, all_rows // act)
    def _(r):
        at = pl.ds(pl.multiple_of(r * act, act), act)
        group = lax.div(r * act, 2 * rows)
        core = lax.rem(lax.div(r * act, rows), 2)
        inside = lax.rem(r * act, rows)
        to = pl.ds(pl.multiple_of(core * 4 * rows + group * rows + inside, act), act)
        for j in range(wide_tiles):
            cols = slice(j * LANES, (j + 1) * LANES)
            gate = acc[at, cols] * gate_rows[j]
            up = acc[at, wide + j * LANES : wide + (j + 1) * LANES] * up_rows[j]
            hid[to, cols] = (gate / (1.0 + jnp.exp(-gate)) * up).astype(bf16)
        both = acc[at, 2 * wide :] * joint_scale
        value = both / (1.0 + jnp.exp(-both)) * pltpu.roll(both, narrow, axis=1)
        keep = lax.broadcasted_iota(jnp.int32, (act, LANES), 1) < narrow
        hid[to, wide:] = jnp.where(keep, value, 0.0).astype(bf16)

    core_rows = all_rows // 2
    own = acc.at[pl.ds(0, core_rows), pl.ds(0, depth)]
    remote(mix_send, mix_recv, half_sem.at[0], half_sem.at[1], to_core).wait_send()
    cut = rows // 2
    chunks = [(i, 0, depth) for i in range(shards - 1)]
    chunks += [(shards - 1, 0, depth // 2), (shards - 1, depth // 2, depth // 2)]
    count = len(chunks)

    def views(i):
        p, at, size = chunks[i]
        return p, p % 2, slice(at, at + size), pl.ds(at, size)

    def slot_at(p):
        return 2 * plane_at(p // 2) + p % 2

    def sems(kind, i):
        p, at, _ = chunks[i]
        j = p % 2 if at == 0 else 2
        send = mix_y.at[3 * kind + j] if kind < 4 else mix_x.at[3 * (kind - 4) + j]
        return send, recv_sem.at[kind * count + i]

    def cs_copy(i):
        p, s, _, ln = views(i)
        source = normed.at[pl.ds(2 * s, 2), :, ln]
        return remote(source, cs_recv.at[p, :, :, ln], *sems(0, i), to_core)

    def bx_copy(i):
        p, s, _, ln = views(i)
        return remote(bx_send.at[s, :, :, ln], bx_recv.at[p, :, :, ln], *sems(1, i), to_x)

    def by_copy(i):
        p, s, _, ln = views(i)
        return remote(by_send.at[s, :, :, ln], by_recv.at[p, :, :, ln], *sems(2, i), to_y)

    def cx_copy(i):
        p, s, _, ln = views(i)
        return remote(cx_send.at[s, :, ln], cx_recv.at[p, :, ln], *sems(3, i), to_x)

    def cy_copy(i):
        p, s, _, ln = views(i)
        return remote(cy_send.at[s, :, ln], cy_recv.at[p, :, ln], *sems(4, i), to_y)

    def out_lanes(i):
        p, at, size = chunks[i]
        return lanes_at(slot_at(p) * depth + at, size)

    def out_copy(i, core=c):
        part = out.at[pl.ds(pl.multiple_of(core * rows, rows), rows), out_lanes(i)]
        return remote(part, part, *sems(5, i), to_core)

    def reused(i, make):
        p, at, _ = chunks[i]
        if p >= 2 and at == 0:
            make(p - 2).wait_send()

    def send_stage(i):
        p, s, cols, _ = views(i)
        slot = slot_at(p)
        reused(i, cs_copy)

        @pl.loop(0, core_rows // tall)
        def _(r):
            there = pl.ds(pl.multiple_of((1 - c) * core_rows + r * tall, tall), tall)
            value = jnp.dot(hid[there, :], dn[slot, :, cols], preferred_element_type=f32)
            normed[2 * s + r, :, cols] = value.astype(bf16)

        cs_copy(i).start()

    def own_stage(i):
        p, _, cols, _ = views(i)
        slot = slot_at(p)

        @pl.loop(0, core_rows // tall)
        def _(r):
            at = pl.ds(pl.multiple_of(r * tall, tall), tall)
            here = pl.ds(pl.multiple_of(c * core_rows + r * tall, tall), tall)
            own[at, cols] = jnp.dot(hid[here, :], dn[slot, :, cols], preferred_element_type=f32)

    def block_rows(bx, by, part):
        first = pl.multiple_of((2 * bx + by) * rows + part * cut, cut)
        inside = pl.multiple_of(by * rows + part * cut, cut)
        return pl.ds(first, cut), bx, pl.ds(inside, cut)

    def second_stage(i):
        p, s, cols, _ = views(i)
        cs_copy(i).wait_recv()
        reused(i, bx_copy)
        reused(i, by_copy)

        def total(block):
            at, pair, inside = block
            return own[at, cols] + cs_recv[p, pair, inside, cols].astype(f32)

        for b in range(2):
            bx_send[s, b, :, cols] = total(block_rows(1 - x, b, 0)).astype(bf16)
        bx_copy(i).start()
        for b in range(2):
            by_send[s, b, :, cols] = total(block_rows(b, 1 - y, 1)).astype(bf16)
        by_copy(i).start()
        for b in range(2):
            keep_l[s, b, :, cols] = total(block_rows(x, b, 0))
            keep_r[s, b, :, cols] = total(block_rows(b, y, 1))

    def third_stage(i):
        p, s, cols, _ = views(i)
        reused(i, cx_copy)
        reused(i, cy_copy)
        bx_copy(i).wait_recv()

        def left(b):
            return keep_l[s, b, :, cols] + bx_recv[p, b, :, cols].astype(f32)

        def right(b):
            return keep_r[s, b, :, cols] + by_recv[p, b, :, cols].astype(f32)

        cy_send[s, :, cols] = left(1 - y).astype(bf16)
        cy_copy(i).start()
        by_copy(i).wait_recv()
        cx_send[s, :, cols] = right(1 - x).astype(bf16)
        cx_copy(i).start()
        last_l[s, :, cols] = left(y)
        last_r[s, :, cols] = right(x)

    def fourth_stage(i):
        p, s, cols, _ = views(i)
        d = slot_at(p)
        scale = scales[d, 1:2, cols]
        for copy, last, recv, at in (
            (cy_copy(i), last_l, cy_recv, slice(0, cut)),
            (cx_copy(i), last_r, cx_recv, slice(cut, rows)),
        ):
            copy.wait_recv()
            total = last[s, :, cols] + recv[p, :, cols].astype(f32)
            value = (mid[d, at, cols].astype(f32) + total * scale).astype(bf16)
            first = pl.multiple_of(c * rows + at.start, cut)
            out[pl.ds(first, cut), out_lanes(i)] = value
        reused(i, out_copy)
        out_copy(i).start()

    stages = {0: send_stage, 1: own_stage, 2: second_stage, 3: third_stage, 4: fourth_stage}
    done = set()

    def run(stage, i):
        if i < 0 or i >= count or (stage, i) in done:
            return
        done.add((stage, i))
        stages[stage](i)

    for i in range(shards - 2):
        if i >= 2:
            for kind in ("dn",) if i % 2 == 0 else ("dna", "dnb"):
                hop(kind, i // 2, i % 2, absolute=True)
        run(0, i)
        run(1, i)
        run(4, i - 4)
        run(3, i - 2)
        run(2, i)
    n = shards - 2
    for stage, i in ((4, n - 4), (3, n - 2), (4, n - 3), (3, n - 1)):
        run(stage, i)
    settle("gu")
    settle("tok")
    hop("dn", planes - 1, 0, absolute=True)
    for stage, i in ((0, n), (1, n), (2, n), (4, n - 2), (4, n - 1)):
        run(stage, i)
    hop("dna", planes - 1, 1, absolute=True)
    for stage, i in ((0, n + 1), (1, n + 1), (2, n + 1)):
        run(stage, i)
    hop("dnb", planes - 1, 1, absolute=True)
    for stage, i in ((0, n + 2), (3, n), (1, n + 2), (2, n + 2), (3, n + 1), (4, n)):
        run(stage, i)
    settle("dn")
    run(3, n + 2)
    run(4, n + 1)
    run(4, n + 2)

    for i in range(shards - 2, count):
        for make in (cs_copy, bx_copy, by_copy, cx_copy, cy_copy, out_copy):
            make(i).wait_send()
    for i in range(count):
        out_copy(i, 1 - c).wait_recv()


def make_fast(shards):
    planes = shards // 2

    def body(
        tokens,
        mixer_gain,
        pool_input,
        input_scale,
        group_mix,
        group_scale,
        pool_output,
        output_scale,
        channel_gain,
        gate_weight,
        gate_scale,
        up_weight,
        up_scale,
        down_weight,
        down_scale,
    ):
        f32, bf16 = jnp.float32, jnp.bfloat16
        length, width = tokens.shape
        depth, local_width = pool_input.shape
        span = gate_weight.shape[1] // 2
        padded = (span // 2 + LANES - 1) // LANES * LANES
        rows = length // 2
        everything = 8 * rows
        anywhere = pl.BlockSpec(memory_space=pl.ANY)
        dma = pltpu.SemaphoreType.DMA
        scratch = [
            pltpu.VMEM((1, width), f32),
            pltpu.VMEM((1, local_width), f32),
            pltpu.VMEM((1, local_width), f32),
            pltpu.VMEM((1, depth), f32),
            pltpu.VMEM((1, width), f32),
            pltpu.VMEM((2 * span // LANES, LANES), f32),
            pltpu.VMEM((2 * span // LANES, LANES), f32),
            pltpu.VMEM((1, depth), f32),
            pltpu.VMEM(group_mix.shape, f32),
            pltpu.VMEM((length, width), bf16),
            pltpu.VMEM((2, shards, depth, local_width), bf16),
            pltpu.VMEM((shards, 2, depth), f32),
            pltpu.VMEM((shards, length, depth), bf16),
            pltpu.VMEM((shards, depth, span), bf16),
            pltpu.VMEM((shards, padded, depth), bf16),
            pltpu.VMEM((depth, span), bf16),
            pltpu.VMEM((span // 2, depth), bf16),
            pltpu.VMEM((shards, everything, depth), bf16),
            pltpu.VMEM((everything, span), f32),
            pltpu.VMEM((everything, padded), bf16),
            pltpu.VMEM((length, local_width), f32),
            pltpu.VMEM((length, local_width), bf16),
            pltpu.VMEM((shards, rows, depth), bf16),
            pltpu.VMEM((shards, rows, depth), bf16),
            pltpu.VMEM((shards, rows, depth), bf16),
            pltpu.VMEM((shards, 2, 2 * rows, depth), bf16),
            pltpu.VMEM((2, 2, rows // 2, depth), bf16),
            pltpu.VMEM((shards, 2, rows // 2, depth), bf16),
            pltpu.VMEM((2, 2, rows // 2, depth), bf16),
            pltpu.VMEM((shards, 2, rows // 2, depth), bf16),
            pltpu.VMEM((2, rows // 2, depth), bf16),
            pltpu.VMEM((shards, rows // 2, depth), bf16),
            pltpu.VMEM((2, rows // 2, depth), bf16),
            pltpu.VMEM((shards, rows // 2, depth), bf16),
            pltpu.VMEM((2, 2, rows // 2, depth), f32),
            pltpu.VMEM((2, 2, rows // 2, depth), f32),
            pltpu.VMEM((2, rows // 2, depth), f32),
            pltpu.VMEM((2, rows // 2, depth), f32),
            dma((6 * (shards + 1),)),
            dma((shards + 2,)),
            dma((shards + 2,)),
            dma((2, shards + 2)),
            dma((shards,)),
            dma((2, shards)),
            dma((2, shards)),
            dma((shards,)),
            dma((shards,)),
            dma((shards + 4,)),
            dma((4,)),
            dma((3,)),
            dma((10,)),
        ]
        row = lambda value: value.reshape(1, -1)
        return pl.pallas_call(
            functools.partial(layer_kernel, planes),
            name="layer",
            out_shape=pltpu.VMEM((length, width), bf16),
            in_specs=[anywhere] * 15,
            out_specs=pl.BlockSpec(memory_space=pltpu.VMEM),
            scratch_shapes=scratch,
            compiler_params=pltpu.CompilerParams(
                collective_id=0, has_side_effects=True, vmem_limit_bytes=60 * 2**20
            ),
        )(
            tokens,
            row(mixer_gain),
            row(input_scale),
            row(group_scale),
            row(output_scale),
            row(channel_gain),
            gate_scale.reshape(-1, LANES),
            up_scale.reshape(-1, LANES),
            row(down_scale),
            group_mix,
            pool_input,
            pool_output,
            gate_weight,
            up_weight,
            down_weight,
        )

    return body


def solution(mesh):
    in_specs = (
        P(("rep", "fs"), None),
        P(),
        P("fs", "tp"),
        P("tp"),
        P(None, "tp"),
        P("tp"),
        P("fs", "tp"),
        P("fs"),
        P(),
        P("fs", "tp"),
        P("tp"),
        P("fs", "tp"),
        P("tp"),
        P("fs", "tp"),
        P("fs"),
    )
    out_specs = P(("rep", "fs"), None)
    reps, shards, cores = mesh.shape["rep"], mesh.shape["fs"], mesh.shape["tp"]
    fast = reps == 2 and cores == 2 and shards % 2 == 0 and shards >= 8
    body = make_fast(shards) if fast else make_body(reps, shards, cores)
    return jax.shard_map(body, mesh=mesh, in_specs=in_specs, out_specs=out_specs, check_vma=False)
```
